32 devices in a mesh: sp: 8 (over z, y), tp: 4 (over x, core).
Axes of the slice: x: 2, y: 2, z: 4, core: 2. Of those that a mesh axis runs over, the one named last changes fastest.
Arguments:
- activations: bfloat16 [4096, 2048], P('sp', 'tp'), may hold values from -250 to 250
- norm_gain: bfloat16 [2048], P('tp'), may hold values from 0.099609375 to 1.8984375
- pool_weight: bfloat16 [2048, 1024], P('sp', 'tp'), may hold values from -0.125 to 0.125
- gate_weight: bfloat16 [2048, 1024], P('sp', 'tp'), may hold values from -0.125 to 0.125
- value_weight: bfloat16 [2048, 1024], P('sp', 'tp'), may hold values from -0.125 to 0.125
- key_weight: bfloat16 [2048, 256], P('sp', 'tp'), may hold values from -0.125 to 0.125
- read_weight: bfloat16 [2048, 256], P('sp', 'tp'), may hold values from -0.125 to 0.125
- step_weight: bfloat16 [2048, 16], P('sp', 'tp'), may hold values from -0.125 to 0.125
- pool_mix: bfloat16 [4, 256, 256], P('tp'), may hold values from -0.375 to 0.375
- pool_scale: float32 [1024], P('tp'), may hold values from 0.1 to 1.9
- taps_value: float32 [4, 1024], P(None, 'tp'), may hold values from -3 to 3
- taps_key: float32 [4, 256], P(None, 'tp'), may hold values from -3 to 3
- taps_read: float32 [4, 256], P(None, 'tp'), may hold values from -3 to 3
- step_bias: float32 [16], P('tp'), may hold values from -1 to 1
- decay_log: float32 [16], P('tp')
- decay_extra: float32 [4096, 16], P('sp', 'tp'), may hold values from -1 to 0
- skip_scale: float32 [16], P('tp'), may hold values from 0.5 to 2
- state_gain: float32 [1024], P('tp'), may hold values from 0.1 to 1.9
- out_pool_weight: bfloat16 [1024, 2048], P('tp', 'sp'), may hold values from -0.125 to 0.125
- out_state_weight: bfloat16 [1024, 2048], P('tp', 'sp'), may hold values from -0.125 to 0.125
Outputs:
- mixed: bfloat16 [4096, 2048], P('sp', 'tp')
The draws below stay inside these ranges and needn't reach their ends.
All inputs are finite; a program needn't handle non-finite values.
Results may differ from the reference program's by a relative error of at most 0.007.
Values may be sent and summed in bfloat16 or wider, within the bound.
A program may use at most 64 MiB of HBM per device.

```python
import math
import jax
import jax.numpy as jnp
from jax import lax

D = 2048
SCAN_HEAD_NUMBER = 16
SSM_HEAD_DIM = 64
SSM_GROUPS = 4
SSM_STATE = 64
POOL_GROUPS = 4
MIXER_CONV_TAPS = 4
SCAN_BLOCK = 128
TOK_DEV = 512
MIX_W = 1024
GW = 256
TOKENS = 4096


def draw_activations(key, part):
    first, second = jax.random.split(key, 2)
    spot = jnp.arange(D).astype(jnp.float32) / D
    rough = jnp.exp(jax.random.uniform(second, (1, D), jnp.float32, -0.35, 0.35))
    basic = jnp.clip(jax.random.normal(first, (TOKENS, D), jnp.float32), -4.0, 4.0)
    rising = jnp.exp(spot * 1.1)[None, :]
    return (basic * rising * rough).astype(jnp.bfloat16)


def draw_decay_log(key, part):
    first, second, third = jax.random.split(key, 3)
    fast_rate = jnp.log(jax.random.uniform(first, (SCAN_HEAD_NUMBER,), jnp.float32, 0.03, 0.1))
    slow_rate = jax.random.uniform(second, (SCAN_HEAD_NUMBER,), jnp.float32, jnp.log(0.1), jnp.log(0.5)) - jnp.log(TOKENS * 1.0)
    chance = 0.5
    quick = jax.random.uniform(third, (SCAN_HEAD_NUMBER,), jnp.float32) < chance
    return jnp.where(quick, fast_rate, slow_rate)


def draw_decay_extra(key, part):
    first, second, third, quarter_slice = jax.random.split(key, 4)
    steady_rate = jnp.exp(jax.random.uniform(first, (1, 1, SCAN_HEAD_NUMBER), jnp.float32, jnp.log(0.2), jnp.log(0.6))) / TOKENS
    factor = jnp.exp(jax.random.uniform(second, (TOKENS // TOK_DEV, 1, 1), jnp.float32, jnp.log(0.25), jnp.log(2.0)))
    constant_baseline = -(factor * steady_rate * jnp.ones((1, TOK_DEV, 1), jnp.float32)).reshape(TOKENS, SCAN_HEAD_NUMBER)
    places = jax.random.randint(third, (3,), 0, TOKENS)
    masked_elements = jnp.any(jnp.arange(TOKENS)[:, None] == places[None, :], axis=1)
    sudden_impulse = jnp.log(jax.random.uniform(quarter_slice, (1, SCAN_HEAD_NUMBER), jnp.float32, 0.5, 0.8))
    return constant_baseline + jnp.where(masked_elements[:, None], sudden_impulse, 0.0)


def shard_levels(key, dims, pieces, least, top_value):
    def one(axis_at, blocks):
        steps = jax.random.uniform(jax.random.fold_in(jax.random.fold_in(key, 6), axis_at), (blocks,), jnp.float32, least / len(pieces), top_value / len(pieces))
        return jnp.repeat(jnp.exp(steps), dims[axis_at] // blocks).reshape((-1,) + (1,) * (len(dims) - axis_at - 1))

    gain = one(*pieces[0])
    for cut in pieces[1:]:
        gain = gain * one(*cut)
    return gain


def normal_values(rng, dims, scale, bound, shards=(), held_as=jnp.bfloat16):
    values = scale * jax.random.normal(rng, dims, jnp.float32)
    if shards:
        values = values * shard_levels(rng, dims, shards, -0.22, 0.18)
    return jnp.clip(values, -bound, bound).astype(held_as)


def setup_inputs(seed: int = 0) -> dict:
    streams_of = jax.random.split(jax.random.key(seed), 21)
    activations = draw_activations(jax.random.fold_in(streams_of[20], 71), 0)
    norm_gain = jnp.clip(1.0 + 0.18 * jax.random.normal(streams_of[1], (D,), jnp.float32), 0.099609375, 1.8984375).astype(jnp.bfloat16)
    pool_weight = normal_values(streams_of[2], (D, MIX_W), D ** -0.5, 0.125, ((0, 8), (1, 4)))
    gate_weight = normal_values(streams_of[3], (D, MIX_W), D ** -0.5, 0.125, ((0, 8), (1, 4)))
    value_weight = normal_values(streams_of[4], (D, MIX_W), D ** -0.5, 0.125, ((0, 8), (1, 4)))
    key_weight = normal_values(streams_of[5], (D, SSM_GROUPS * SSM_STATE), D ** -0.5, 0.125, ((0, 8), (1, 4)))
    read_weight = normal_values(streams_of[6], (D, SSM_GROUPS * SSM_STATE), D ** -0.5, 0.125, ((0, 8), (1, 4)))
    step_weight = normal_values(streams_of[7], (D, SCAN_HEAD_NUMBER), D ** -0.5, 0.125, ((0, 8), (1, 4)))
    pool_mix = normal_values(streams_of[8], (POOL_GROUPS, GW, GW), GW ** -0.5, 0.375, ((0, 4),))
    pool_scale = jnp.clip(1.0 + 0.18 * jax.random.normal(streams_of[9], (MIX_W,), jnp.float32), 0.1, 1.9)
    taps_value = normal_values(streams_of[10], (MIXER_CONV_TAPS, MIX_W), MIXER_CONV_TAPS ** -0.5, 3.0, ((1, 4),), jnp.float32)
    taps_key = normal_values(streams_of[11], (MIXER_CONV_TAPS, SSM_GROUPS * SSM_STATE), MIXER_CONV_TAPS ** -0.5, 3.0, ((1, 4),), jnp.float32)
    taps_read = normal_values(streams_of[12], (MIXER_CONV_TAPS, SSM_GROUPS * SSM_STATE), MIXER_CONV_TAPS ** -0.5, 3.0, ((1, 4),), jnp.float32)
    step_bias = jnp.clip(jax.random.uniform(streams_of[13], (SCAN_HEAD_NUMBER,), jnp.float32, -1.0, 1.0) * shard_levels(streams_of[13], (SCAN_HEAD_NUMBER,), ((0, 4),), -0.4, 0.0), -1.0, 1.0)
    decay_log = draw_decay_log(jax.random.fold_in(streams_of[20], 71), 0)
    decay_extra = draw_decay_extra(jax.random.fold_in(streams_of[20], 71), 0)
    skip_scale = jnp.clip(jnp.exp(math.log(2.0) - 1.3862944 * jax.random.uniform(streams_of[16], (SCAN_HEAD_NUMBER,), jnp.float32) ** shard_levels(streams_of[16], (SCAN_HEAD_NUMBER,), ((0, 4),), -0.2, 0.2)), 0.5, 2.0)
    state_gain = jnp.clip(1.0 + 0.18 * jax.random.normal(streams_of[17], (MIX_W,), jnp.float32), 0.1, 1.9)
    out_pool_weight = normal_values(streams_of[18], (MIX_W, D), (2 * MIX_W) ** -0.5, 0.125, ((0, 4), (1, 8)))
    out_state_weight = normal_values(streams_of[19], (MIX_W, D), (2 * MIX_W) ** -0.5, 0.125, ((0, 4), (1, 8)))
    return {"activations": activations, "norm_gain": norm_gain, "pool_weight": pool_weight, "gate_weight": gate_weight, "value_weight": value_weight, "key_weight": key_weight, "read_weight": read_weight, "step_weight": step_weight, "pool_mix": pool_mix, "pool_scale": pool_scale, "taps_value": taps_value, "taps_key": taps_key, "taps_read": taps_read, "step_bias": step_bias, "decay_log": decay_log, "decay_extra": decay_extra, "skip_scale": skip_scale, "state_gain": state_gain, "out_pool_weight": out_pool_weight, "out_state_weight": out_state_weight}


EPSILON = 1e-06
HIGH = lax.Precision.HIGHEST

def backward_kernel(raw, taps):
    width = taps.shape[0]
    length = raw.shape[0]
    padded = jnp.pad(raw.astype(jnp.float32), ((width - 1, 0), (0, 0)))
    total = jnp.zeros(raw.shape, jnp.float32)
    for offset in range(width):
        total = total + taps[offset][None, :] * padded[offset:offset + length]
    return jax.nn.silu(total).astype(jnp.bfloat16)

def scan_block(state, inputs):
    head_value, step_size, log_decay, key_heads, read_heads = inputs
    length = head_value.shape[0]
    running = jnp.cumsum(log_decay, axis=0)
    lower = jnp.arange(length)[:, None] >= jnp.arange(length)[None, :]
    gaps = jnp.where(lower[:, :, None], running[:, None, :] - running[None, :, :], -jnp.inf)
    weights = jnp.einsum('lhn,shn->lsh', read_heads, key_heads, precision=HIGH) * jnp.exp(gaps)
    scaled_value = head_value * step_size[:, :, None]
    inner = jnp.einsum('lsh,shp->lhp', weights, scaled_value, precision=HIGH)
    carried = jnp.einsum('lhn,hpn->lhp', read_heads, state, precision=HIGH) * jnp.exp(running)[:, :, None]
    trailing = jnp.exp(running[-1][None, :] - running)
    fresh = jnp.einsum('shn,sh,shp->hpn', key_heads, trailing, scaled_value, precision=HIGH)
    new_state = state * jnp.exp(running[-1])[:, None, None] + fresh
    return (new_state, inner + carried)

def reference(activations, norm_gain, pool_weight, gate_weight, value_weight, key_weight, read_weight, step_weight, pool_mix, pool_scale, taps_value, taps_key, taps_read, step_bias, decay_log, decay_extra, skip_scale, state_gain, out_pool_weight, out_state_weight):
    values = activations.astype(jnp.float32)
    normed = (values * lax.rsqrt(lax.optimization_barrier(jnp.mean(values * values, axis=-1, keepdims=True)) + EPSILON) * norm_gain.astype(jnp.float32)).astype(jnp.bfloat16)
    pool_in = jnp.dot(normed, pool_weight, preferred_element_type=jnp.float32).astype(jnp.bfloat16)
    gate_in = jnp.dot(normed, gate_weight, preferred_element_type=jnp.float32).astype(jnp.bfloat16)
    raw_value = jnp.dot(normed, value_weight, preferred_element_type=jnp.float32).astype(jnp.bfloat16)
    raw_key = jnp.dot(normed, key_weight, preferred_element_type=jnp.float32).astype(jnp.bfloat16)
    raw_read = jnp.dot(normed, read_weight, preferred_element_type=jnp.float32).astype(jnp.bfloat16)
    step_raw = jnp.dot(normed, step_weight, preferred_element_type=jnp.float32)
    reach = 2 ** POOL_GROUPS - 1
    pool_values = pool_in.astype(jnp.float32)
    padded = jnp.pad(pool_values, ((reach, 0), (0, 0)))
    position = jnp.arange(TOKENS).astype(jnp.float32)
    outputs = []
    for group in range(POOL_GROUPS):
        window = 2 ** (group + 1)
        column_count = padded[:, group * GW:(group + 1) * GW]
        window_sum = jnp.zeros((TOKENS, GW), jnp.float32)
        for back in range(window):
            window_sum = window_sum + column_count[reach - back:reach - back + TOKENS]
        counts = jnp.minimum(position + 1.0, float(window))
        pooled = (window_sum / counts[:, None] - pool_values[:, group * GW:(group + 1) * GW]).astype(jnp.bfloat16)
        outputs.append(jnp.dot(pooled, pool_mix[group], preferred_element_type=jnp.float32))
    pool_out = (jnp.concatenate(outputs, axis=1) * pool_scale).astype(jnp.bfloat16)
    head_value = backward_kernel(raw_value, taps_value)
    key_vectors = backward_kernel(raw_key, taps_key)
    read_vectors = backward_kernel(raw_read, taps_read)
    step_size = jax.nn.softplus(step_raw + step_bias)
    log_decay = -jnp.exp(decay_log) * step_size + decay_extra
    repeat = SCAN_HEAD_NUMBER // SSM_GROUPS
    blocks = TOKENS // SCAN_BLOCK
    value_heads = head_value.astype(jnp.float32).reshape(TOKENS, SCAN_HEAD_NUMBER, SSM_HEAD_DIM)
    key_heads = jnp.repeat(key_vectors.astype(jnp.float32).reshape(TOKENS, SSM_GROUPS, SSM_STATE), repeat, axis=1)
    read_heads = jnp.repeat(read_vectors.astype(jnp.float32).reshape(TOKENS, SSM_GROUPS, SSM_STATE), repeat, axis=1)
    start = jnp.zeros((SCAN_HEAD_NUMBER, SSM_HEAD_DIM, SSM_STATE), jnp.float32)
    _, scanned = lax.scan(scan_block, start, (value_heads.reshape(blocks, SCAN_BLOCK, SCAN_HEAD_NUMBER, SSM_HEAD_DIM), step_size.reshape(blocks, SCAN_BLOCK, SCAN_HEAD_NUMBER), log_decay.reshape(blocks, SCAN_BLOCK, SCAN_HEAD_NUMBER), key_heads.reshape(blocks, SCAN_BLOCK, SCAN_HEAD_NUMBER, SSM_STATE), read_heads.reshape(blocks, SCAN_BLOCK, SCAN_HEAD_NUMBER, SSM_STATE)))
    scan_out = scanned.reshape(TOKENS, SCAN_HEAD_NUMBER, SSM_HEAD_DIM) + skip_scale[None, :, None] * value_heads
    gated = scan_out.reshape(TOKENS, MIX_W) * jax.nn.silu(gate_in.astype(jnp.float32))
    state_out = (gated * lax.rsqrt(lax.optimization_barrier(jnp.mean(gated * gated, axis=-1, keepdims=True)) + EPSILON) * state_gain).astype(jnp.bfloat16)
    result = jnp.dot(pool_out, out_pool_weight, preferred_element_type=jnp.float32) + jnp.dot(state_out, out_state_weight, preferred_element_type=jnp.float32)
    return result.astype(jnp.bfloat16)
```

```python
import functools

import jax
import jax.numpy as jnp
from jax import lax
from jax.experimental import pallas as pl
from jax.experimental.pallas import tpu as pltpu
from jax.sharding import PartitionSpec as P

SSM_STATE = 64
POOL_GROUPS = 4
SCAN_BLOCK = 128
MIX_W = 1024


EPSILON = 1e-06
HIGH = lax.Precision.HIGHEST


def shifted(value, axis, steps):
    count = lax.axis_size(axis)
    leading, last = (max(0, -steps), min(count, count - steps))
    return lax.ppermute(value, axis, [(source, source + steps) for source in range(leading, last)])


def carried_in(part, axis, combine, identity):
    place = lax.axis_index(axis)
    gathered = jax.tree.map(lambda a: lax.all_gather(a, axis), part)
    state = jax.tree.map(lambda a, e: jnp.zeros_like(a) + jnp.asarray(e, a.dtype), part, identity)

    def one(step, state):
        return combine(
            state, jax.tree.map(lambda a: lax.dynamic_index_in_dim(a, step, 0, False), gathered)
        )

    return lax.fori_loop(0, place, one, state)


def backward_kernel(extended, taps):
    width = taps.shape[0]
    length = extended.shape[0] - (width - 1)
    widened_rows = extended.astype(jnp.float32)
    total = jnp.zeros((length, extended.shape[1]), jnp.float32)
    for offset in range(width):
        total = total + taps[offset][None, :] * widened_rows[offset : offset + length]
    return jax.nn.silu(total).astype(jnp.bfloat16)


def combine_states(preceding_token, later):
    return (preceding_token[0] * later[0], preceding_token[1] * later[0][:, None, None] + later[1])


def local(
    activations,
    norm_gain,
    pool_weight,
    gate_weight,
    value_weight,
    key_weight,
    read_weight,
    step_weight,
    pool_mix,
    pool_scale,
    taps_value,
    taps_key,
    taps_read,
    step_bias,
    decay_log,
    decay_extra,
    skip_scale,
    state_gain,
    out_pool_weight,
    out_state_weight,
):
    length = activations.shape[0]
    cluster_span = pool_weight.shape[1]
    local_mix = gate_weight.shape[1]
    local_state = key_weight.shape[1]
    local_heads = step_weight.shape[1]
    joined = jnp.concatenate(
        [pool_weight, gate_weight, value_weight, key_weight, read_weight, step_weight], axis=1
    )
    in_weight = lax.all_gather(joined, "sp", axis=0, tiled=True)
    whole, gains = (
        lax.all_gather(activations, "tp", axis=1, tiled=True),
        lax.all_gather(norm_gain, "tp", axis=0, tiled=True),
    )
    widened_rows = whole.astype(jnp.float32)
    normed = (
        widened_rows
        * lax.rsqrt(jnp.mean(widened_rows * widened_rows, axis=-1, keepdims=True) + EPSILON)
        * gains.astype(jnp.float32)
    ).astype(jnp.bfloat16)
    projected = jnp.dot(normed, in_weight, preferred_element_type=jnp.float32)
    column = 0
    pool_in = projected[:, column : column + cluster_span].astype(jnp.bfloat16)
    column = column + cluster_span
    gate_in = projected[:, column : column + local_mix].astype(jnp.bfloat16)
    column = column + local_mix
    raw_value = projected[:, column : column + local_mix].astype(jnp.bfloat16)
    column = column + local_mix
    raw_key = projected[:, column : column + local_state].astype(jnp.bfloat16)
    column = column + local_state
    raw_read = projected[:, column : column + local_state].astype(jnp.bfloat16)
    column = column + local_state
    step_raw = projected[:, column : column + local_heads]
    raw_joined = jnp.concatenate([raw_value, raw_key, raw_read], axis=1)
    reach = 2**POOL_GROUPS - 1
    width = taps_value.shape[0]
    prior_pool, prior_joined = shifted(
        (pool_in[length - reach :], raw_joined[length - width + 1 :]), "sp", 1
    )
    group = lax.axis_index("tp")
    running = jnp.concatenate([prior_pool, pool_in], axis=0).astype(jnp.float32)
    levels = []
    for level in range(POOL_GROUPS):
        stride = 2**level
        running = running[stride:] + running[:-stride]
        levels.append(running[running.shape[0] - length :])
    window_sum = lax.dynamic_index_in_dim(jnp.stack(levels), group, 0, keepdims=False)
    window = jnp.exp2((group + 1).astype(jnp.float32))
    position = (lax.axis_index("sp") * length + jnp.arange(length, dtype=jnp.int32)).astype(
        jnp.float32
    )
    counts = jnp.minimum(position + 1.0, window)
    pooled = (window_sum / counts[:, None] - pool_in.astype(jnp.float32)).astype(jnp.bfloat16)
    pool_out = (
        jnp.dot(pooled, pool_mix[0], preferred_element_type=jnp.float32) * pool_scale
    ).astype(jnp.bfloat16)
    all_taps = jnp.concatenate([taps_value, taps_key, taps_read], axis=1)
    convolved = backward_kernel(jnp.concatenate([prior_joined, raw_joined], axis=0), all_taps)
    head_value = convolved[:, :local_mix]
    key_vectors = convolved[:, local_mix : local_mix + local_state]
    read_vectors = convolved[:, local_mix + local_state :]
    head_dim = local_mix // local_heads
    groups_here = local_state // SSM_STATE
    repeat = local_heads // groups_here
    blocks = length // SCAN_BLOCK
    step_size = jax.nn.softplus(step_raw + step_bias)
    log_decay = -jnp.exp(decay_log) * step_size + decay_extra
    value_heads = head_value.astype(jnp.float32).reshape(length, local_heads, head_dim)
    value_blocks = value_heads.reshape(blocks, SCAN_BLOCK, local_heads, head_dim)
    key_blocks = jnp.repeat(
        key_vectors.astype(jnp.float32).reshape(length, groups_here, SSM_STATE), repeat, axis=1
    ).reshape(blocks, SCAN_BLOCK, local_heads, SSM_STATE)
    read_blocks = jnp.repeat(
        read_vectors.astype(jnp.float32).reshape(length, groups_here, SSM_STATE), repeat, axis=1
    ).reshape(blocks, SCAN_BLOCK, local_heads, SSM_STATE)
    step_blocks = step_size.reshape(blocks, SCAN_BLOCK, local_heads)
    running_decay = jnp.cumsum(log_decay.reshape(blocks, SCAN_BLOCK, local_heads), axis=1)
    lower = jnp.arange(SCAN_BLOCK)[:, None] >= jnp.arange(SCAN_BLOCK)[None, :]
    gaps = jnp.where(
        lower[None, :, :, None],
        running_decay[:, :, None, :] - running_decay[:, None, :, :],
        -jnp.inf,
    )
    weights = jnp.einsum("blhn,bshn->blsh", read_blocks, key_blocks, precision=HIGH) * jnp.exp(gaps)
    scaled_value = value_blocks * step_blocks[..., None]
    inner = jnp.einsum("blsh,bshp->blhp", weights, scaled_value, precision=HIGH)
    block_ends = running_decay[:, -1, :]
    trailing = jnp.exp(block_ends[:, None, :] - running_decay)
    fresh = jnp.einsum("bshn,bsh,bshp->bhpn", key_blocks, trailing, scaled_value, precision=HIGH)

    def advance(carry, inputs):
        block_decay, block_state = inputs
        return (carry * block_decay[:, None, None] + block_state, carry)

    local_total, prefix = lax.scan(
        advance,
        jnp.zeros((local_heads, head_dim, SSM_STATE), jnp.float32),
        (jnp.exp(block_ends), fresh),
    )
    offsets = jnp.cumsum(block_ends, axis=0) - block_ends
    device_decay = jnp.exp(offsets[-1] + block_ends[-1])
    incoming_decay, incoming = carried_in(
        (device_decay, local_total),
        "sp",
        combine_states,
        (jnp.ones_like(device_decay), jnp.zeros_like(local_total)),
    )
    from_device = running_decay + offsets[:, None, :]
    local_off = (
        jnp.einsum("blhn,bhpn->blhp", read_blocks, prefix, precision=HIGH)
        * jnp.exp(running_decay)[..., None]
    )
    far_off = (
        jnp.einsum("blhn,hpn->blhp", read_blocks, incoming, precision=HIGH)
        * jnp.exp(from_device)[..., None]
    )
    scan_out = (inner + local_off + far_off).reshape(length, local_heads, head_dim) + skip_scale[
        None, :, None
    ] * value_heads
    gated = scan_out.reshape(length, local_mix) * jax.nn.silu(gate_in.astype(jnp.float32))
    gate_squares = lax.psum(jnp.sum(gated * gated, axis=-1), "tp")
    state_out = (gated * lax.rsqrt(gate_squares / MIX_W + EPSILON)[:, None] * state_gain).astype(
        jnp.bfloat16
    )
    branch_rows = jnp.concatenate([pool_out, state_out], axis=1)
    out_weight = jnp.concatenate([out_pool_weight, out_state_weight], axis=0)
    terms = jnp.dot(
        branch_rows,
        lax.all_gather(out_weight, "sp", axis=1, tiled=True),
        preferred_element_type=jnp.float32,
    )
    result = lax.psum_scatter(terms, "tp", scatter_dimension=1, tiled=True)
    return result.astype(jnp.bfloat16)


BF = jnp.bfloat16
F32 = jnp.float32
MESH = pl.DeviceIdType.MESH


def flip(index, mask):
    bit = 1
    while bit <= mask:
        if mask & bit:
            index = index + bit - 2 * bit * lax.rem(lax.div(index, bit), 2)
        bit *= 2
    return index


def bt(a, b, **kw):
    return lax.dot_general(a, b, (((1,), (1,)), ((), ())), preferred_element_type=F32, **kw)


def halves(x):
    top = x.astype(BF)
    return top, (x - top.astype(F32)).astype(BF)


def mixer_kernel(
    S, T,
    act, gain, pool_w, gate_w, value_w, key_w, read_w, step_t, mix, scale, taps_v, taps_k, taps_r,
    bias, dlog, extra_t, skip, sgain, opool, ostate,
    out,
    vbuf, gbuf, obuf, abuf, mixb, par, nbuf, extv, extp, gateb, conv, hvs, hvr, hps, hpr, scan, xs, xr,
    sq_buf, pbuf, sbuf, expd,
    b_ss, b_rs, o_ss, o_rs, a_ss, a_rs, t_ss, t_rs, h_ss, h_rs, x_ss, x_rs, q_ss, q_rs, p_ss, p_rs,
):
    n, da = act.shape
    kd, cw = pool_w.shape
    st = key_w.shape[0]
    heads = step_t.shape[0]
    hp = vbuf.shape[1] - kd
    vc = cw + 2 * st
    oc = opool.shape[1]
    blk = SCAN_BLOCK
    blocks = n // blk
    hd = SSM_STATE
    Z = S // 2
    sp, tq = lax.axis_index("sp"), lax.axis_index("tp")
    z, y = lax.div(sp, 2), lax.rem(sp, 2)
    x, c = lax.div(tq, 2), lax.rem(tq, 2)
    me, tp = 2 * z + c, 2 * x + y
    off = lax.rem(y + c, 2)
    moved, kept = off == 1, off == 0
    slot = me + off * (S - me)
    aslot = tq + off * (T - tq)
    pslot = tp + off * (T - tp)
    hub = tq == z
    oslot = jnp.where(hub, y * T + tq, 2 * T)

    def dev(z_=z, y_=y, x_=x, c_=c):
        return {"sp": 2 * z_ + y_, "tp": 2 * x_ + c_}

    def copy(src, dst, ss, rs, **to):
        return pltpu.make_async_remote_copy(
            src_ref=src, dst_ref=dst, send_sem=ss, recv_sem=rs, device_id=dev(**to), device_id_type=MESH
        )

    eye_kd = jnp.where(
        lax.broadcasted_iota(jnp.int32, (kd, kd), 0) == lax.broadcasted_iota(jnp.int32, (kd, kd), 1), 1.0, 0.0
    ).astype(BF)
    pick = jnp.where(
        lax.broadcasted_iota(jnp.int32, (hp, heads), 0) == lax.broadcasted_iota(jnp.int32, (hp, heads), 1), 1.0, 0.0
    ).astype(F32)
    vbuf[slot, 0:kd, 0:cw] = value_w[...]
    vbuf[slot, 0:kd, cw:] = bt(eye_kd, jnp.concatenate([key_w[...], read_w[...]], axis=0)).astype(BF)
    vbuf[slot, kd:, :] = jnp.zeros((hp, vc), BF)
    vbuf[slot, kd:, 0:kd] = jnp.dot(pick.astype(BF), step_t[...], preferred_element_type=F32).astype(BF)
    abuf[aslot, 0:n, :] = act[...]
    abuf[aslot, n : n + 16, :] = jnp.broadcast_to(gain[...].astype(F32), (16, da)).astype(BF)

    barrier = pltpu.get_barrier_semaphore()

    def greet(**to):
        pl.semaphore_signal(barrier, inc=1, device_id=dev(**to), device_id_type=MESH)

    for k in range(1, 8):
        greet(
            y_=1 - y if k & 4 else y, x_=1 - x if k & 2 else x, c_=1 - c if k & 1 else c,
        )
    for k in range(1, Z):
        greet(z_=lax.rem(z + k, Z))
        greet(z_=lax.rem(z + k, Z), c_=1 - c)
    gbuf[slot, :, 0:cw] = pool_w[...]
    gbuf[slot, :, cw:] = gate_w[...]
    obuf[oslot, 0:cw, :] = opool[...]
    obuf[oslot, cw:, :] = ostate[...]
    mixb[off] = mix[0]
    par[off] = jnp.zeros(par.shape[1:], F32)
    par[off, 0:heads, :] = extra_t[...]
    par[off, 16:17, 0:cw] = scale[...]
    par[off, 16:17, cw : 2 * cw] = sgain[...]
    par[off, 17:18, 0:heads] = bias[...]
    par[off, 18:19, 0:heads] = dlog[...]
    par[off, 19:20, 0:heads] = skip[...]
    width = taps_v.shape[0]
    par[off, 24 : 24 + width, 0:cw] = taps_v[...]
    par[off, 24 : 24 + width, cw : cw + st] = taps_k[...]
    par[off, 24 : 24 + width, cw + st : vc] = taps_r[...]
    pl.semaphore_wait(barrier, 7 + 2 * (Z - 1))

    streams = (vbuf, gbuf)

    def bcopy(k, i, way):
        to = ({"c_": 1 - c}, {"z_": z + 1}, {"z_": z - 1})[way]
        ref = streams[k].at[i]
        return copy(ref, ref, b_ss.at[(k * S + i) * 3 + way], b_rs.at[k * S + i], **to)

    def arrived(k, i):
        bcopy(k, i, 0).wait_recv()

    def source(k, do):
        @pl.when(z < Z - 1)
        def _():
            do(bcopy(k, me, 1))

        @pl.when(z > 0)
        def _():
            do(bcopy(k, me, 2))

        do(bcopy(k, me, 0))

    def start(d):
        d.start()

    def done(d):
        d.wait_send()

    def pump(k, d, do, wait=True):
        @pl.when(z >= d)
        def _():
            i = 2 * (z - d) + c
            if wait:
                arrived(k, i)

            @pl.when(z < Z - 1)
            def _():
                do(bcopy(k, i, 1))

            do(bcopy(k, i, 0))

        @pl.when(z + d < Z)
        def _():
            i = 2 * (z + d) + c
            if wait:
                arrived(k, i)

            @pl.when(z > 0)
            def _():
                do(bcopy(k, i, 2))

            do(bcopy(k, i, 0))

    def partners(k):
        for p in range(Z):
            arrived(k, 2 * p + 1 - c)

    def swap(i):
        src, dst, rs = (
            (vbuf.at[S], vbuf.at[sp], b_rs.at[sp]),
            (par.at[1], par.at[0], t_rs.at[0]),
            (gbuf.at[S], gbuf.at[sp], b_rs.at[S + sp]),
            (mixb.at[1], mixb.at[0], t_rs.at[1]),
        )[i]
        return copy(src, dst, t_ss.at[i], rs, y_=c, c_=y)

    def acopy(way):
        to = ({"c_": y}, {"x_": 1 - x, "c_": y}, {"y_": 1 - y, "c_": y})[way]
        return copy(abuf.at[aslot], abuf.at[tq], a_ss.at[way], a_rs.at[tq], **to)

    def aforward(f):
        t = 2 * x + f
        return copy(abuf.at[t], abuf.at[t], a_ss.at[3 + f], a_rs.at[t], x_=1 - x)

    def agot(t):
        copy(abuf.at[t], abuf.at[t], a_ss.at[0], a_rs.at[t], x_=1 - x).wait_recv()

    def ohub():
        return copy(
            obuf.at[2 * T], obuf.at[y * T + tq], o_ss.at[0], o_rs.at[y * T + tq], x_=lax.div(z, 2), c_=lax.rem(z, 2)
        )

    def ocopy(q, way):
        to = ({"y_": 1 - y}, {"z_": z + 1}, {"z_": z - 1})[way]
        ref = obuf.at[y * T + q]
        return copy(ref, ref, o_ss.at[1 + q * 3 + way], o_rs.at[y * T + q], **to)

    def omoves(q, do):
        @pl.when((z >= tq) & (z < Z - 1))
        def _():
            do(ocopy(q, 1))

        @pl.when((z <= tq) & (z > 0))
        def _():
            do(ocopy(q, 2))

        do(ocopy(q, 0))

    def oslice(tau):
        for q in range(T):
            d = tau - q
            if d == 0:
                @pl.when(hub)
                def _():
                    @pl.when(tq != q)
                    def _():
                        ocopy(q, 0).wait_recv()

                    omoves(q, start)
            elif 0 < d < Z:
                @pl.when((z == tq + d) | (z == tq - d))
                def _():
                    ocopy(q, 0).wait_recv()
                    omoves(q, start)

    @pl.when(moved)
    def _():
        swap(0).start()

    acopy(1).start()
    acopy(2).start()

    @pl.when(moved)
    def _():
        acopy(0).start()
        for i in range(1, 4):
            swap(i).start()

    @pl.when(jnp.logical_not(hub))
    def _():
        ohub().start()

    @pl.when(moved)
    def _():
        arrived(0, me)

    source(0, start)

    @pl.when(kept)
    def _():
        source(1, start)

    @pl.when(moved)
    def _():
        agot(2 * x + c)
        aforward(c).start()

    pump(0, 1, start)

    @pl.when(moved)
    def _():
        agot(2 * x + 1 - c)
        aforward(1 - c).start()

    pump(0, 2, start)

    @pl.when(moved)
    def _():
        arrived(1, me)
        source(1, start)

    oslice(0)
    pump(1, 1, start)
    pump(0, 3, start)
    partners(0)

    @pl.when(kept)
    def _():
        agot(2 * x + 1 - c)

    agot(2 * (1 - x))
    agot(2 * (1 - x) + 1)

    per = da // kd
    rt = 64

    def norm_rows(i, _):
        r = pl.ds(pl.multiple_of(i * rt, rt), rt)
        parts = [abuf[t, r, :].astype(F32) for t in range(T)]
        tot = sum(jnp.sum(p * p, axis=-1, keepdims=True) for p in parts)
        rs = lax.rsqrt(tot / (da * T) + EPSILON)
        for t in range(T):
            g = abuf[t, n : n + 1, :].astype(F32)
            v = (parts[t] * rs * g).astype(BF)
            for j in range(per):
                nbuf[t * per + j, r, :] = v[:, j * kd : (j + 1) * kd]
        return 0

    lax.fori_loop(0, n // rt, norm_rows, 0)
    mt = 256
    raw0 = 16

    for r0 in range(0, n, mt):
        d = jnp.dot(nbuf[0, r0 : r0 + mt, :], vbuf[0, 0:kd, :], preferred_element_type=F32)
        for i in range(1, S):
            d = d + jnp.dot(nbuf[i, r0 : r0 + mt, :], vbuf[i, 0:kd, :], preferred_element_type=F32)
        low = d.astype(BF)
        extv[raw0 + r0 : raw0 + r0 + mt, :] = low.astype(F32)
        if r0 + mt == n:
            hvs[...] = low[mt - raw0 :, :]

    def halo(src, dst, i):
        return copy(src, dst, h_ss.at[i], h_rs.at[i], z_=z + c, c_=1 - c)

    @pl.when(me < S - 1)
    def _():
        halo(hvs, hvr, 0).start()

    sacc = bt(vbuf[0, kd:, 0:kd], nbuf[0])
    for i in range(1, S):
        sacc = sacc + bt(vbuf[i, kd:, 0:kd], nbuf[i])
    oslice(1)
    pump(1, 2, start)

    @pl.when(moved)
    def _():
        swap(1).wait_recv()
        swap(3).wait_recv()

    def column(row):
        return bt(pick, jnp.broadcast_to(row, (8, heads)), precision=HIGH)[:, 0:1]

    step = sacc + column(par[0, 17:18, 0:heads])
    step = jnp.maximum(step, 0.0) + jnp.log1p(jnp.exp(-jnp.abs(step)))
    ld = -jnp.exp(column(par[0, 18:19, 0:heads])) * step + par[0, 0:hp, :]
    r_i = lax.broadcasted_iota(jnp.int32, (blk, blk), 0)
    c_i = lax.broadcasted_iota(jnp.int32, (blk, blk), 1)
    upper = jnp.where(r_i <= c_i, 1.0, 0.0).astype(F32)
    eye = jnp.where(r_i == c_i, 1.0, 0.0).astype(F32)
    lower = r_i >= c_i
    expand = jnp.where(
        lax.broadcasted_iota(jnp.int32, (hp, cw), 1) // hd == lax.broadcasted_iota(jnp.int32, (hp, cw), 0), 1.0, 0.0
    ).astype(F32)
    skips = jnp.dot(
        jnp.broadcast_to(par[0, 19:20, 0:heads], (8, heads)), expand[0:heads, :],
        precision=HIGH, preferred_element_type=F32,
    )[0:1, :]
    eye_st = jnp.where(
        lax.broadcasted_iota(jnp.int32, (st, st), 0) == lax.broadcasted_iota(jnp.int32, (st, st), 1), 1.0, 0.0
    ).astype(BF)
    cum_rs, cum_cs, st_rs, wexps = [], [], [], []
    for b in range(blocks):
        cols = slice(b * blk, (b + 1) * blk)
        cum_r = jnp.dot(ld[:, cols], upper, precision=HIGH, preferred_element_type=F32)
        st_r = step[:, cols]
        turned = bt(eye, jnp.concatenate([cum_r, st_r], axis=0), precision=HIGH)
        cum_c = turned[:, 0:hp]
        w_c = jnp.exp(cum_c[blk - 1 : blk, :] - cum_c) * turned[:, hp:]
        both = jnp.dot(
            jnp.concatenate([w_c, jnp.exp(cum_c)], axis=0), expand, precision=HIGH, preferred_element_type=F32
        )
        expd[cols, :] = both[blk:, :]
        wexps.append(both[:blk, :])
        cum_rs.append(cum_r)
        cum_cs.append(cum_c)
        st_rs.append(st_r)

    oslice(2)

    @pl.when(me > 0)
    def _():
        halo(hvs, hvr, 0).wait_recv()
        extv[0:raw0, :] = hvr[...].astype(F32)

    @pl.when(me == 0)
    def _():
        extv[0:raw0, :] = jnp.zeros((raw0, vc), F32)

    for b in range(blocks):
        for lo, hi in ((0, cw), (cw, vc)):
            total = jnp.zeros((blk, hi - lo), F32)
            for k in range(width):
                o = b * blk + raw0 - (width - 1) + k
                total = total + par[0, 24 + k : 25 + k, lo:hi] * extv[o : o + blk, lo:hi]
            conv[b * blk : (b + 1) * blk, lo:hi] = (total * jax.nn.sigmoid(total)).astype(BF)

    run = jnp.zeros((st, cw), F32)
    dec = jnp.ones((1, cw), F32)
    pres, offs = [], []
    for b in range(blocks):
        rows = slice(b * blk, (b + 1) * blk)
        key_t = bt(eye_st, conv[rows, cw : cw + st]).astype(BF)
        sv = conv[rows, 0:cw].astype(F32) * wexps[b]
        top, low = halves(sv)
        new = jnp.dot(key_t, top, preferred_element_type=F32) + jnp.dot(key_t, low, preferred_element_type=F32)
        bd = expd[(b + 1) * blk - 1 : (b + 1) * blk, :]
        pres.append(run)
        offs.append(dec)
        run = run * bd + new
        dec = dec * bd

    in_s = jnp.zeros((st, cw), F32)
    in_d = jnp.ones((1, cw), F32)
    rounds = [1 << k for k in range(S.bit_length() - 1)]

    def inner(b):
        rows = slice(b * blk, (b + 1) * blk)
        g = bt(conv[rows, cw + st :], conv[rows, cw : cw + st])
        for h in range(cw // hd):
            gap = jnp.where(lower, cum_cs[b][:, h : h + 1] - cum_rs[b][h : h + 1, :], -jnp.inf)
            wm = g * jnp.exp(gap) * st_rs[b][h : h + 1, :]
            top, low = halves(wm)
            v = conv[rows, h * hd : (h + 1) * hd]
            scan[rows, h * hd : (h + 1) * hd] = jnp.dot(top, v, preferred_element_type=F32) + jnp.dot(
                low, v, preferred_element_type=F32
            )

    window = lax.shift_left(jnp.int32(2), tp)
    back = (
        lax.broadcasted_iota(jnp.int32, (blk, blk + raw0), 0)
        + raw0
        - lax.broadcasted_iota(jnp.int32, (blk, blk + raw0), 1)
    )
    band = jnp.where((back >= 0) & (back < window), 1.0, 0.0).astype(BF)

    def pool(b):
        rows = slice(b * blk, (b + 1) * blk)
        sums = jnp.dot(band, extp[b * blk : (b + 1) * blk + raw0, :].astype(BF), preferred_element_type=F32)
        pos = (me * n + b * blk + lax.broadcasted_iota(jnp.int32, (blk, cw), 0)).astype(F32)
        counts = jnp.minimum(pos + 1.0, window.astype(F32))
        pooled = (sums / counts - extp[b * blk + raw0 : (b + 1) * blk + raw0, :]).astype(BF)
        pbuf[pslot, rows, :] = (
            jnp.dot(pooled, mixb[0], preferred_element_type=F32) * par[0, 16:17, 0:cw]
        ).astype(BF)

    def xpeer(bit):
        return {"c_": 1 - c} if bit == 1 else {"z_": flip(z, bit // 2)}

    work = [functools.partial(inner, b) for b in range(blocks)]
    share = -(-len(work) // len(rounds))
    for r, bit in enumerate(rounds):
        xs[r, 0:st, :] = run
        xs[r, st:, :] = jnp.broadcast_to(dec, (xs.shape[1] - st, cw))
        copy(xs.at[r], xr.at[r], x_ss.at[r], x_rs.at[r], **xpeer(bit)).start()
        for f in work[r * share : (r + 1) * share]:
            f()
        if r == 0:
            oslice(3)
            pump(1, 3, start)
        if r == 1:
            oslice(4)
        copy(xs.at[r], xr.at[r], x_ss.at[r], x_rs.at[r], **xpeer(bit)).wait_recv()
        other, odec = xr[r, 0:st, :], xr[r, st : st + 1, :]
        later = lax.rem(lax.div(me, bit), 2) == 1
        in_s = jnp.where(later, other * in_d + in_s, in_s)
        in_d = jnp.where(later, odec * in_d, in_d)
        run = jnp.where(later, other * dec + run, run * odec + other)
        dec = dec * odec

    for b in range(blocks):
        rows = slice(b * blk, (b + 1) * blk)
        top, low = halves(pres[b] + offs[b] * in_s)
        rd = conv[rows, cw + st :]
        carried = jnp.dot(rd, top, preferred_element_type=F32) + jnp.dot(rd, low, preferred_element_type=F32)
        scan[rows, :] = scan[rows, :] + carried * expd[rows, :] + skips * conv[rows, 0:cw].astype(F32)

    partners(1)
    for r0 in range(0, n, mt):
        d = jnp.dot(nbuf[0, r0 : r0 + mt, :], gbuf[0], preferred_element_type=F32)
        for i in range(1, S):
            d = d + jnp.dot(nbuf[i, r0 : r0 + mt, :], gbuf[i], preferred_element_type=F32)
        low = d.astype(BF)
        extp[raw0 + r0 : raw0 + r0 + mt, :] = low[:, 0:cw].astype(F32)
        gateb[r0 : r0 + mt, :] = low[:, cw:]
        if r0 + mt == n:
            hps[...] = low[mt - raw0 :, 0:cw]

    @pl.when(me < S - 1)
    def _():
        halo(hps, hpr, 1).start()

    for b in range(blocks):
        rows = slice(b * blk, (b + 1) * blk)
        gt = gateb[rows, :].astype(F32)
        gated = scan[rows, :] * (gt * jax.nn.sigmoid(gt))
        sq_buf[pslot, :, rows] = bt(jnp.ones((8, cw), F32), gated * gated, precision=HIGH)
        sbuf[pslot, rows, :] = (gated * par[0, 16:17, cw : 2 * cw]).astype(BF)

    rows_of = (sbuf, pbuf)

    def rcopy(k, r, way, src=None):
        to = ({"c_": 1 - c}, {"x_": 1 - x}, {"y_": 1 - y})[way]
        src = rows_of[k].at[r] if src is None else src
        return copy(src, rows_of[k].at[r], p_ss.at[(k * T + r) * 3 + way], p_rs.at[k * T + r], **to)

    def qcopy(i):
        to = ({"c_": 1 - c}, {"x_": 1 - x}, {"x_": 1 - x, "c_": 1 - c}, {})[i]
        return copy(sq_buf.at[pslot], sq_buf.at[tp], q_ss.at[i], q_rs.at[tp], **{"y_": c, **to})

    def rows_out(k, do):
        @pl.when(moved)
        def _():
            do(rcopy(k, tp, 2, rows_of[k].at[T]))

        @pl.when(kept)
        def _():
            do(rcopy(k, tp, 1))
            do(rcopy(k, tp, 0))

    def rows_on(k, do, wait=True):
        @pl.when(kept)
        def _():
            other = 2 * x + 1 - y
            if wait:
                rcopy(k, other, 0).wait_recv()
            do(rcopy(k, other, 1))
            do(rcopy(k, other, 0))
            for r in (2 * (1 - x) + y, 2 * (1 - x) + 1 - y):
                if wait:
                    rcopy(k, r, 0).wait_recv()
                do(rcopy(k, r, 0))

    def squares(do):
        for i in range(3):
            do(qcopy(i))

        @pl.when(moved)
        def _():
            do(qcopy(3))

    squares(start)
    rows_out(0, start)
    oslice(5)

    @pl.when(me > 0)
    def _():
        halo(hps, hpr, 1).wait_recv()
        extp[0:raw0, :] = hpr[...].astype(F32)

    @pl.when(me == 0)
    def _():
        extp[0:raw0, :] = jnp.zeros((raw0, cw), F32)

    for b in range(blocks):
        pool(b)
    rows_out(1, start)
    rows_on(0, start)
    oslice(6)
    rows_on(1, start)

    @pl.when(moved)
    def _():
        for k in range(2):
            for r in range(T):
                rcopy(k, r, 0).wait_recv()

    for r in range(T):
        @pl.when((tp != r) | moved)
        def _():
            copy(sq_buf.at[r], sq_buf.at[r], q_ss.at[0], q_rs.at[r], c_=1 - c).wait_recv()

    for q in range(T):
        ref = obuf.at[(1 - y) * T + q]
        copy(ref, ref, o_ss.at[0], o_rs.at[(1 - y) * T + q], y_=1 - y).wait_recv()

    sq = sum(sq_buf[r] for r in range(T))
    rs_row = lax.rsqrt(sq / (cw * T) + EPSILON)
    rs_cols = [bt(eye, rs_row[:, b * blk : (b + 1) * blk], precision=HIGH)[:, 0:1] for b in range(blocks)]
    for r0 in range(0, n, mt):
        rows = slice(r0, r0 + mt)
        rs = jnp.concatenate(rs_cols[r0 // blk : (r0 + mt) // blk], axis=0)
        for j in range(2):
            p = jnp.dot(pbuf[0, rows, :], obuf[j * T, 0:cw, :], preferred_element_type=F32)
            s = jnp.dot(sbuf[0, rows, :], obuf[j * T, cw:, :], preferred_element_type=F32)
            for q in range(1, T):
                p = p + jnp.dot(pbuf[q, rows, :], obuf[j * T + q, 0:cw, :], preferred_element_type=F32)
                s = s + jnp.dot(sbuf[q, rows, :], obuf[j * T + q, cw:, :], preferred_element_type=F32)
            out[rows, j * oc : (j + 1) * oc] = (p + rs * s).astype(out.dtype)

    for k in range(2):
        source(k, done)
        for d in range(1, Z):
            pump(k, d, done, wait=False)
        rows_out(k, done)
        rows_on(k, done, wait=False)
    for q in range(T):
        omoves(q, done)
    squares(done)
    acopy(1).wait_send()
    acopy(2).wait_send()

    @pl.when(moved)
    def _():
        acopy(0).wait_send()
        for i in range(4):
            swap(i).wait_send()
        for f in range(2):
            aforward(f).wait_send()

    @pl.when(jnp.logical_not(hub))
    def _():
        ohub().wait_send()

    for r, bit in enumerate(rounds):
        copy(xs.at[r], xr.at[r], x_ss.at[r], x_rs.at[r], **xpeer(bit)).wait_send()

    @pl.when(me < S - 1)
    def _():
        halo(hvs, hvr, 0).wait_send()
        halo(hps, hpr, 1).wait_send()


def fits(S, T, shapes):
    n, da = shapes[0]
    kd, cw = shapes[2]
    st = shapes[5][1]
    oc = shapes[18][1]
    heads = shapes[7][1]
    taps = shapes[10][0]
    return (
        T == 4 == POOL_GROUPS and S == 2 * T and st == SSM_STATE and taps <= 8 and heads <= 8
        and cw == heads * SSM_STATE and n % 256 == 0 and n % SCAN_BLOCK == 0 and n >= 2 * cw
        and oc % 128 == 0 and kd % 128 == 0 and da % kd == 0 and da * T == kd * S and kd <= cw + 2 * st
        and cw % 128 == 0 and oc * 2 == da
    )


def fused(
    S, T, activations, norm_gain, pool_weight, gate_weight, value_weight, key_weight, read_weight,
    step_weight, pool_mix, pool_scale, taps_value, taps_key, taps_read, step_bias, decay_log,
    decay_extra, skip_scale, state_gain, out_pool_weight, out_state_weight,
):
    n, da = activations.shape
    kd, cw = pool_weight.shape
    st = key_weight.shape[1]
    oc = out_pool_weight.shape[1]
    hp = 16
    args = (
        activations, norm_gain[None, :], pool_weight, gate_weight, value_weight, key_weight.T, read_weight.T,
        step_weight.T, pool_mix, pool_scale[None, :], taps_value, taps_key, taps_read, step_bias[None, :], decay_log[None, :],
        decay_extra.T, skip_scale[None, :], state_gain[None, :],
        out_pool_weight, out_state_weight,
    )
    vc = cw + 2 * st
    V = pltpu.VMEM
    D = pltpu.SemaphoreType.DMA
    R = S.bit_length() - 1
    scratch = [
        V((S + 1, kd + hp, vc), BF), V((S + 1, kd, 2 * cw), BF), V((2 * T + 1, 2 * cw, oc), BF),
        V((T + 1, n + 16, da), BF), V((2, cw, cw), BF), V((2, 32, n), F32),
        V((S, n, kd), BF), V((n + 16, vc), F32), V((n + 16, cw), F32), V((n, cw), BF), V((n, vc), BF),
        V((16, vc), BF), V((16, vc), BF), V((16, cw), BF), V((16, cw), BF), V((n, cw), F32),
        V((R, st + 8, cw), F32), V((R, st + 8, cw), F32),
        V((T + 1, 8, n), F32), V((T + 1, n, cw), BF), V((T + 1, n, cw), BF), V((n, cw), F32),
        D((6 * S,)), D((2 * S,)), D((1 + 3 * T,)), D((2 * T,)), D((5,)), D((T,)), D((4,)), D((2,)),
        D((2,)), D((2,)), D((R,)), D((R,)), D((4,)), D((T,)), D((6 * T,)), D((2 * T,)),
    ]
    return pl.pallas_call(
        functools.partial(mixer_kernel, S, T),
        out_shape=jax.ShapeDtypeStruct((n, da), BF),
        in_specs=[pl.BlockSpec(memory_space=pltpu.VMEM)] * len(args),
        out_specs=pl.BlockSpec(memory_space=pltpu.VMEM),
        scratch_shapes=scratch,
        compiler_params=pltpu.CompilerParams(
            collective_id=0, has_side_effects=True, vmem_limit_bytes=60 * 1024 * 1024
        ),
    )(*args)


def solution(mesh):
    placed = (
        P("sp", "tp"),
        P("tp"),
        P("sp", "tp"),
        P("sp", "tp"),
        P("sp", "tp"),
        P("sp", "tp"),
        P("sp", "tp"),
        P("sp", "tp"),
        P("tp", None, None),
        P("tp"),
        P(None, "tp"),
        P(None, "tp"),
        P(None, "tp"),
        P("tp"),
        P("tp"),
        P("sp", "tp"),
        P("tp"),
        P("tp"),
        P("tp", "sp"),
        P("tp", "sp"),
    )
    S, T = mesh.shape["sp"], mesh.shape["tp"]

    def chosen(*args):
        if fits(S, T, [a.shape for a in args]):
            return fused(S, T, *args)
        return local(*args)

    return jax.shard_map(
        chosen, mesh=mesh, in_specs=placed, out_specs=P("sp", "tp"), check_vma=False
    )
```

```python
import functools

import jax
import jax.numpy as jnp
from jax import lax
from jax.experimental import pallas as pl
from jax.experimental.pallas import tpu as pltpu
from jax.sharding import PartitionSpec as P

SSM_STATE = 64
POOL_GROUPS = 4
SCAN_BLOCK = 128
MIX_W = 1024


EPSILON = 1e-06
HIGH = lax.Precision.HIGHEST


def shifted(value, axis, steps):
    count = lax.axis_size(axis)
    leading, last = (max(0, -steps), min(count, count - steps))
    return lax.ppermute(value, axis, [(source, source + steps) for source in range(leading, last)])


def carried_in(part, axis, combine, identity):
    place = lax.axis_index(axis)
    gathered = jax.tree.map(lambda a: lax.all_gather(a, axis), part)
    state = jax.tree.map(lambda a, e: jnp.zeros_like(a) + jnp.asarray(e, a.dtype), part, identity)

    def one(step, state):
        return combine(
            state, jax.tree.map(lambda a: lax.dynamic_index_in_dim(a, step, 0, False), gathered)
        )

    return lax.fori_loop(0, place, one, state)


def backward_kernel(extended, taps):
    width = taps.shape[0]
    length = extended.shape[0] - (width - 1)
    widened_rows = extended.astype(jnp.float32)
    total = jnp.zeros((length, extended.shape[1]), jnp.float32)
    for offset in range(width):
        total = total + taps[offset][None, :] * widened_rows[offset : offset + length]
    return jax.nn.silu(total).astype(jnp.bfloat16)


def combine_states(preceding_token, later):
    return (preceding_token[0] * later[0], preceding_token[1] * later[0][:, None, None] + later[1])


def local(
    activations,
    norm_gain,
    pool_weight,
    gate_weight,
    value_weight,
    key_weight,
    read_weight,
    step_weight,
    pool_mix,
    pool_scale,
    taps_value,
    taps_key,
    taps_read,
    step_bias,
    decay_log,
    decay_extra,
    skip_scale,
    state_gain,
    out_pool_weight,
    out_state_weight,
):
    length = activations.shape[0]
    cluster_span = pool_weight.shape[1]
    local_mix = gate_weight.shape[1]
    local_state = key_weight.shape[1]
    local_heads = step_weight.shape[1]
    joined = jnp.concatenate(
        [pool_weight, gate_weight, value_weight, key_weight, read_weight, step_weight], axis=1
    )
    in_weight = lax.all_gather(joined, "sp", axis=0, tiled=True)
    whole, gains = (
        lax.all_gather(activations, "tp", axis=1, tiled=True),
        lax.all_gather(norm_gain, "tp", axis=0, tiled=True),
    )
    widened_rows = whole.astype(jnp.float32)
    normed = (
        widened_rows
        * lax.rsqrt(jnp.mean(widened_rows * widened_rows, axis=-1, keepdims=True) + EPSILON)
        * gains.astype(jnp.float32)
    ).astype(jnp.bfloat16)
    projected = jnp.dot(normed, in_weight, preferred_element_type=jnp.float32)
    column = 0
    pool_in = projected[:, column : column + cluster_span].astype(jnp.bfloat16)
    column = column + cluster_span
    gate_in = projected[:, column : column + local_mix].astype(jnp.bfloat16)
    column = column + local_mix
    raw_value = projected[:, column : column + local_mix].astype(jnp.bfloat16)
    column = column + local_mix
    raw_key = projected[:, column : column + local_state].astype(jnp.bfloat16)
    column = column + local_state
    raw_read = projected[:, column : column + local_state].astype(jnp.bfloat16)
    column = column + local_state
    step_raw = projected[:, column : column + local_heads]
    raw_joined = jnp.concatenate([raw_value, raw_key, raw_read], axis=1)
    reach = 2**POOL_GROUPS - 1
    width = taps_value.shape[0]
    prior_pool, prior_joined = shifted(
        (pool_in[length - reach :], raw_joined[length - width + 1 :]), "sp", 1
    )
    group = lax.axis_index("tp")
    running = jnp.concatenate([prior_pool, pool_in], axis=0).astype(jnp.float32)
    levels = []
    for level in range(POOL_GROUPS):
        stride = 2**level
        running = running[stride:] + running[:-stride]
        levels.append(running[running.shape[0] - length :])
    window_sum = lax.dynamic_index_in_dim(jnp.stack(levels), group, 0, keepdims=False)
    window = jnp.exp2((group + 1).astype(jnp.float32))
    position = (lax.axis_index("sp") * length + jnp.arange(length, dtype=jnp.int32)).astype(
        jnp.float32
    )
    counts = jnp.minimum(position + 1.0, window)
    pooled = (window_sum / counts[:, None] - pool_in.astype(jnp.float32)).astype(jnp.bfloat16)
    pool_out = (
        jnp.dot(pooled, pool_mix[0], preferred_element_type=jnp.float32) * pool_scale
    ).astype(jnp.bfloat16)
    all_taps = jnp.concatenate([taps_value, taps_key, taps_read], axis=1)
    convolved = backward_kernel(jnp.concatenate([prior_joined, raw_joined], axis=0), all_taps)
    head_value = convolved[:, :local_mix]
    key_vectors = convolved[:, local_mix : local_mix + local_state]
    read_vectors = convolved[:, local_mix + local_state :]
    head_dim = local_mix // local_heads
    groups_here = local_state // SSM_STATE
    repeat = local_heads // groups_here
    blocks = length // SCAN_BLOCK
    step_size = jax.nn.softplus(step_raw + step_bias)
    log_decay = -jnp.exp(decay_log) * step_size + decay_extra
    value_heads = head_value.astype(jnp.float32).reshape(length, local_heads, head_dim)
    value_blocks = value_heads.reshape(blocks, SCAN_BLOCK, local_heads, head_dim)
    key_blocks = jnp.repeat(
        key_vectors.astype(jnp.float32).reshape(length, groups_here, SSM_STATE), repeat, axis=1
    ).reshape(blocks, SCAN_BLOCK, local_heads, SSM_STATE)
    read_blocks = jnp.repeat(
        read_vectors.astype(jnp.float32).reshape(length, groups_here, SSM_STATE), repeat, axis=1
    ).reshape(blocks, SCAN_BLOCK, local_heads, SSM_STATE)
    step_blocks = step_size.reshape(blocks, SCAN_BLOCK, local_heads)
    running_decay = jnp.cumsum(log_decay.reshape(blocks, SCAN_BLOCK, local_heads), axis=1)
    lower = jnp.arange(SCAN_BLOCK)[:, None] >= jnp.arange(SCAN_BLOCK)[None, :]
    gaps = jnp.where(
        lower[None, :, :, None],
        running_decay[:, :, None, :] - running_decay[:, None, :, :],
        -jnp.inf,
    )
    weights = jnp.einsum("blhn,bshn->blsh", read_blocks, key_blocks, precision=HIGH) * jnp.exp(gaps)
    scaled_value = value_blocks * step_blocks[..., None]
    inner = jnp.einsum("blsh,bshp->blhp", weights, scaled_value, precision=HIGH)
    block_ends = running_decay[:, -1, :]
    trailing = jnp.exp(block_ends[:, None, :] - running_decay)
    fresh = jnp.einsum("bshn,bsh,bshp->bhpn", key_blocks, trailing, scaled_value, precision=HIGH)

    def advance(carry, inputs):
        block_decay, block_state = inputs
        return (carry * block_decay[:, None, None] + block_state, carry)

    local_total, prefix = lax.scan(
        advance,
        jnp.zeros((local_heads, head_dim, SSM_STATE), jnp.float32),
        (jnp.exp(block_ends), fresh),
    )
    offsets = jnp.cumsum(block_ends, axis=0) - block_ends
    device_decay = jnp.exp(offsets[-1] + block_ends[-1])
    incoming_decay, incoming = carried_in(
        (device_decay, local_total),
        "sp",
        combine_states,
        (jnp.ones_like(device_decay), jnp.zeros_like(local_total)),
    )
    from_device = running_decay + offsets[:, None, :]
    local_off = (
        jnp.einsum("blhn,bhpn->blhp", read_blocks, prefix, precision=HIGH)
        * jnp.exp(running_decay)[..., None]
    )
    far_off = (
        jnp.einsum("blhn,hpn->blhp", read_blocks, incoming, precision=HIGH)
        * jnp.exp(from_device)[..., None]
    )
    scan_out = (inner + local_off + far_off).reshape(length, local_heads, head_dim) + skip_scale[
        None, :, None
    ] * value_heads
    gated = scan_out.reshape(length, local_mix) * jax.nn.silu(gate_in.astype(jnp.float32))
    gate_squares = lax.psum(jnp.sum(gated * gated, axis=-1), "tp")
    state_out = (gated * lax.rsqrt(gate_squares / MIX_W + EPSILON)[:, None] * state_gain).astype(
        jnp.bfloat16
    )
    branch_rows = jnp.concatenate([pool_out, state_out], axis=1)
    out_weight = jnp.concatenate([out_pool_weight, out_state_weight], axis=0)
    terms = jnp.dot(
        branch_rows,
        lax.all_gather(out_weight, "sp", axis=1, tiled=True),
        preferred_element_type=jnp.float32,
    )
    result = lax.psum_scatter(terms, "tp", scatter_dimension=1, tiled=True)
    return result.astype(jnp.bfloat16)


BF = jnp.bfloat16
F32 = jnp.float32
MESH = pl.DeviceIdType.MESH


def flip(index, mask):
    bit = 1
    while bit <= mask:
        if mask & bit:
            index = index + bit - 2 * bit * lax.rem(lax.div(index, bit), 2)
        bit *= 2
    return index


def bt(a, b, **kw):
    return lax.dot_general(a, b, (((1,), (1,)), ((), ())), preferred_element_type=F32, **kw)


def halves(x):
    top = x.astype(BF)
    return top, (x - top.astype(F32)).astype(BF)


def mixer_kernel(
    S, T,
    act, gain, pool_w, gate_w, value_w, key_w, read_w, step_t, mix, scale, taps_v, taps_k, taps_r,
    bias, dlog, extra_t, skip, sgain, opool, ostate,
    out,
    vbuf, gbuf, obuf, abuf, mixb, par, nbuf, extv, extp, gateb, conv, hbuf, scan, xs, xr,
    sq_buf, pbuf, sbuf, expd,
    b_ss, b_rs, o_ss, o_rs, a_ss, a_rs, t_ss, t_rs, h_ss, h_rs, x_ss, x_rs, q_ss, q_rs, p_ss, p_rs,
):
    n, da = act.shape
    kd, cw = pool_w.shape
    st = key_w.shape[0]
    heads = step_t.shape[0]
    hp = vbuf.shape[1] - kd
    vc = cw + 2 * st
    oc = opool.shape[1]
    blk = SCAN_BLOCK
    blocks = n // blk
    hd = SSM_STATE
    Z = S // 2
    sp, tq = lax.axis_index("sp"), lax.axis_index("tp")
    z, y = lax.div(sp, 2), lax.rem(sp, 2)
    x, c = lax.div(tq, 2), lax.rem(tq, 2)
    me, tp = 2 * z + c, 2 * x + y
    off = lax.rem(y + c, 2)
    moved, kept = off == 1, off == 0
    slot = me + off * (S - me)
    aslot = tq + off * (T - tq)
    pslot = tp + off * (T - tp)
    hubs = (tq == z, 2 * (1 - x) + c == z)
    hub = hubs[0] | hubs[1]
    turn = lax.rem(y + c, 2)
    oslot = jnp.where(hubs[0], y * T + tq, jnp.where(hubs[1], 2 * T + 1 + turn, 2 * T))

    def dev(z_=z, y_=y, x_=x, c_=c):
        return {"sp": 2 * z_ + y_, "tp": 2 * x_ + c_}

    def copy(src, dst, ss, rs, **to):
        return pltpu.make_async_remote_copy(
            src_ref=src, dst_ref=dst, send_sem=ss, recv_sem=rs, device_id=dev(**to), device_id_type=MESH
        )

    barrier = pltpu.get_barrier_semaphore()

    def greet(**to):
        pl.semaphore_signal(barrier, inc=1, device_id=dev(**to), device_id_type=MESH)

    for dz in range(Z):
        for k in range(8):
            if dz or k:
                greet(
                    z_=lax.rem(z + dz, Z), y_=1 - y if k & 4 else y, x_=1 - x if k & 2 else x,
                    c_=1 - c if k & 1 else c,
                )

    eye_kd = jnp.where(
        lax.broadcasted_iota(jnp.int32, (kd, kd), 0) == lax.broadcasted_iota(jnp.int32, (kd, kd), 1), 1.0, 0.0
    ).astype(BF)
    pick = jnp.where(
        lax.broadcasted_iota(jnp.int32, (hp, heads), 0) == lax.broadcasted_iota(jnp.int32, (hp, heads), 1), 1.0, 0.0
    ).astype(F32)
    vbuf[slot, 0:kd, 0:cw] = value_w[...]
    vbuf[slot, 0:kd, cw:] = bt(eye_kd, jnp.concatenate([key_w[...], read_w[...]], axis=0)).astype(BF)
    vbuf[slot, kd:, :] = jnp.zeros((hp, vc), BF)
    vbuf[slot, kd:, 0:kd] = jnp.dot(pick.astype(BF), step_t[...], preferred_element_type=F32).astype(BF)
    abuf[aslot, 0:n, :] = act[...]
    abuf[aslot, n : n + 16, :] = jnp.broadcast_to(gain[...].astype(F32), (16, da)).astype(BF)

    gbuf[slot, :, 0:cw] = pool_w[...]
    gbuf[slot, :, cw:] = gate_w[...]
    obuf[oslot, 0:cw, :] = opool[...]
    obuf[oslot, cw:, :] = ostate[...]
    mixb[off] = mix[0]
    par[off] = jnp.zeros(par.shape[1:], F32)
    par[off, 0:heads, :] = extra_t[...]
    par[off, 16:17, 0:cw] = scale[...]
    par[off, 16:17, cw : 2 * cw] = sgain[...]
    par[off, 17:18, 0:heads] = bias[...]
    par[off, 18:19, 0:heads] = dlog[...]
    par[off, 19:20, 0:heads] = skip[...]
    width = taps_v.shape[0]
    par[off, 24 : 24 + width, 0:cw] = taps_v[...]
    par[off, 24 : 24 + width, cw : cw + st] = taps_k[...]
    par[off, 24 : 24 + width, cw + st : vc] = taps_r[...]
    pl.semaphore_wait(barrier, S * T - 1)

    raw0 = hbuf.shape[1]
    own_halo = (y == 0) & (c == 1)

    @pl.when(own_halo)
    def _():
        hbuf[tq] = act[n - raw0 :, :]

    @pl.when(me == 0)
    def _():
        hbuf[...] = jnp.zeros(hbuf.shape, BF)

    middle = (z == 1) | (z == Z - 2)
    streams = (vbuf, gbuf)

    def bcopy(k, i, way):
        to = ({"c_": 1 - c}, {"z_": z + 1}, {"z_": z - 1}, {"z_": z + 2}, {"z_": z - 2})[way]
        ref = streams[k].at[i]
        return copy(ref, ref, b_ss.at[(k * S + i) * 5 + way], b_rs.at[k * S + i], **to)

    def arrived(k, i):
        bcopy(k, i, 0).wait_recv()

    def source(k, do):
        ways = [(1, z < Z - 1), (2, z > 0)]
        if k:
            ways = [(3, moved & (z == 0)), (4, moved & (z == Z - 1))] + ways
        for way, when in ways:
            @pl.when(when)
            def _():
                do(bcopy(k, me, way))

        do(bcopy(k, me, 0))

    def start(d):
        d.start()

    def done(d):
        d.wait_send()

    def pump(k, d, do, wait=True, when=True):
        right, left = z < Z - 1, z > 0
        if k and d == 1:
            right, left = right & (kept | (z > 1)), left & (kept | (z < Z - 2))

        @pl.when((z >= d) & when)
        def _():
            i = 2 * (z - d) + c
            if wait:
                arrived(k, i)

            @pl.when(right)
            def _():
                do(bcopy(k, i, 1))

            do(bcopy(k, i, 0))

        @pl.when((z + d < Z) & when)
        def _():
            i = 2 * (z + d) + c
            if wait:
                arrived(k, i)

            @pl.when(left)
            def _():
                do(bcopy(k, i, 2))

            do(bcopy(k, i, 0))

    def partners(k):
        for p in range(Z):
            arrived(k, 2 * p + 1 - c)

    def swap(i):
        src, dst, rs = (
            (vbuf.at[S], vbuf.at[sp], b_rs.at[sp]),
            (par.at[1], par.at[0], t_rs.at[0]),
            (gbuf.at[S], gbuf.at[sp], b_rs.at[S + sp]),
            (mixb.at[1], mixb.at[0], t_rs.at[1]),
        )[i]
        return copy(src, dst, t_ss.at[i], rs, y_=c, c_=y)

    def acopy(way):
        to = ({"c_": y}, {"x_": 1 - x, "c_": y}, {"y_": 1 - y, "c_": y})[way]
        return copy(abuf.at[aslot], abuf.at[tq], a_ss.at[way], a_rs.at[tq], **to)

    def aforward(i):
        t, to = ((2 * x + 1 - c, {"x_": 1 - x}), (2 * (1 - x) + c, {"y_": 1 - y}))[i]
        return copy(abuf.at[t], abuf.at[t], a_ss.at[3 + i], a_rs.at[t], **to)

    def agot(t):
        copy(abuf.at[t], abuf.at[t], a_ss.at[0], a_rs.at[t], x_=1 - x).wait_recv()

    def hcopy(k):
        return copy(
            abuf.at[aslot, pl.ds(n - raw0, raw0)], hbuf.at[tq], h_ss.at[k], h_rs.at[tq],
            z_=z + y, y_=k // 2, x_=k % 2, c_=1 - y,
        )

    def hsends(do):
        @pl.when(sp < S - 1)
        def _():
            for k in range(4):
                @pl.when(jnp.logical_not(own_halo & (y == k // 2) & (x == k % 2)))
                def _():
                    do(hcopy(k))

    def hgot():
        @pl.when(me > 0)
        def _():
            for t in range(T):
                @pl.when(jnp.logical_not(own_halo & (tq == t)))
                def _():
                    copy(hbuf.at[t], hbuf.at[t], h_ss.at[0], h_rs.at[t], x_=1 - x).wait_recv()

    def oquarter(j):
        return 2 * x + (y if j == 0 else 1 - y)

    def oslots(line, j):
        return 2 * T + 1 + j if line else y * T + oquarter(j)

    def ohub():
        home = lax.div(z, 2) == x
        dst = jnp.where(home, y * T + tq, 2 * T + 1 + turn)
        return copy(obuf.at[2 * T], obuf.at[dst], o_ss.at[0], o_rs.at[dst], c_=1 - c)

    def ocopy(line, j, way):
        to = (
            {"z_": z + 1}, {"z_": z - 1}, {"z_": z + 2}, {"z_": z - 2},
            {"x_": 1 - x} if line else {"y_": 1 - y},
        )[way]
        i = oslots(line, j)
        dst = i if way < 4 else y * T + oquarter(j)
        return copy(obuf.at[i], obuf.at[dst], o_ss.at[1 + (2 * line + j) * 6 + way], o_rs.at[dst], **to)

    def owait(line, j):
        i = oslots(line, j)
        copy(obuf.at[i], obuf.at[i], o_ss.at[0], o_rs.at[i], x_=1 - x).wait_recv()

    def across(line, j, do):
        if not line:
            do(ocopy(line, j, 4))

    def over(line, j, do):
        if line:
            do(ocopy(line, j, 4))

    def osend(line, j, do):
        for way, when in ((2, z == 0), (3, z == Z - 1), (0, middle), (1, middle)):
            @pl.when(when)
            def _():
                do(ocopy(line, j, way))

    def center(line):
        return 2 * (1 - x) + c if line else tq

    def relays(line):
        h = center(line)
        return ((z == Z - 2) & (h < 2)) | ((z == 1) & (h > 1))

    def orelay(line, j, do):
        h = center(line)
        for way, when in ((0, h < 2), (1, h > 1), (1, h == 0), (0, h == T - 1)):
            @pl.when(when)
            def _():
                do(ocopy(line, j, way))

    def ofrom(j, when=True):
        for line in range(2):
            @pl.when(hubs[line] & when)
            def _():
                osend(line, j, start)

    def ocross():
        for line in range(2):
            @pl.when(hubs[line])
            def _():
                for j in range(2):
                    @pl.when(turn != j)
                    def _():
                        owait(line, j)

                    over(line, j, start)
                    across(line, j, start)

    def opass(j):
        for line in range(2):
            @pl.when(relays(line))
            def _():
                owait(line, j)
                orelay(line, j, start)
                over(line, j, start)

                @pl.when(kept)
                def _():
                    across(line, j, start)

    def olate():
        for line in range(2):
            @pl.when(relays(line) & moved)
            def _():
                for j in range(2):
                    across(line, j, start)

    def oend(line, j):
        @pl.when(jnp.logical_not(hubs[line] | relays(line)))
        def _():
            owait(line, j)
            over(line, j, start)
            across(line, j, start)

    def ofar(j, do, wait=True):
        i = y * T + 2 * (1 - x) + (y if j == 0 else 1 - y)
        d = copy(obuf.at[i], obuf.at[i], o_ss.at[25 + j], o_rs.at[i], y_=1 - y)
        if wait:
            d.wait_recv()
        do(d)

    def oall(do):
        for j in range(2):
            ofar(j, do, False)

        for line in range(2):
            for j in range(2):
                @pl.when(hubs[line])
                def _():
                    osend(line, j, do)

                @pl.when(relays(line))
                def _():
                    orelay(line, j, do)

                over(line, j, do)
                across(line, j, do)

    @pl.when(moved)
    def _():
        swap(0).start()

    acopy(1).start()
    hsends(start)

    @pl.when(moved)
    def _():
        acopy(2).start()
        acopy(0).start()
        swap(2).start()

        @pl.when(jnp.logical_not(hub))
        def _():
            ohub().start()

    @pl.when(moved)
    def _():
        arrived(0, me)

    source(0, start)

    @pl.when(kept)
    def _():
        source(1, start)

    pump(0, 1, start)

    @pl.when(kept)
    def _():
        acopy(2).start()
        agot(2 * (1 - x) + c)
        aforward(1).start()

        @pl.when(jnp.logical_not(hub))
        def _():
            ohub().start()

    @pl.when(moved)
    def _():
        agot(2 * x + 1 - c)
        aforward(0).start()

    pump(0, 2, start)

    pump(0, 3, start)

    @pl.when(moved)
    def _():
        swap(1).start()
        swap(3).start()
        arrived(1, me)
        source(1, start)

    @pl.when(kept)
    def _():
        pump(1, 1, start)

    partners(0)

    @pl.when(kept)
    def _():
        agot(2 * x + 1 - c)

    @pl.when(moved)
    def _():
        agot(2 * x + c)
        agot(2 * (1 - x) + c)

    agot(2 * (1 - x) + 1 - c)
    hgot()

    ocross()
    per = da // kd
    rt = 64

    def norm_rows(parts, r):
        tot = sum(jnp.sum(p * p, axis=-1, keepdims=True) for p in parts)
        rs = lax.rsqrt(tot / (da * T) + EPSILON)
        for t in range(T):
            g = abuf[t, n : n + 1, :].astype(F32)
            v = (parts[t] * rs * g).astype(BF)
            for j in range(per):
                nbuf[t * per + j, r, :] = v[:, j * kd : (j + 1) * kd]

    def norm_tile(i, _):
        r = pl.ds(pl.multiple_of(i * rt, rt), rt)
        norm_rows([abuf[t, r, :].astype(F32) for t in range(T)], r)
        return 0

    lax.fori_loop(0, n // rt, norm_tile, 0)
    norm_rows([hbuf[t].astype(F32) for t in range(T)], pl.ds(n, raw0))
    @pl.when(moved)
    def _():
        pump(1, 1, start)


    mt = 256

    def tiles():
        for r0 in range(0, n, mt):
            yield r0, slice(r0, r0 + mt + raw0 if r0 + mt == n else r0 + mt)

    def keep(ref, r0, low):
        ref[raw0 + r0 : raw0 + r0 + mt, :] = low[0:mt, :].astype(F32)
        if low.shape[0] > mt:
            ref[0:raw0, :] = low[mt:, :].astype(F32)

    for r0, rows in tiles():
        d = jnp.dot(nbuf[0, rows, :], vbuf[0, 0:kd, :], preferred_element_type=F32)
        for i in range(1, S):
            d = d + jnp.dot(nbuf[i, rows, :], vbuf[i, 0:kd, :], preferred_element_type=F32)
        keep(extv, r0, d.astype(BF))

    sacc = bt(vbuf[0, kd:, 0:kd], nbuf[0, 0:n, :])
    for i in range(1, S):
        sacc = sacc + bt(vbuf[i, kd:, 0:kd], nbuf[i, 0:n, :])
    @pl.when(kept)
    def _():
        pump(1, 2, start)

    @pl.when(moved)
    def _():
        pump(1, 2, start, when=middle)

    ofrom(0)

    @pl.when(moved)
    def _():
        swap(1).wait_recv()
        swap(3).wait_recv()

    def column(row):
        return bt(pick, jnp.broadcast_to(row, (8, heads)), precision=HIGH)[:, 0:1]

    step = sacc + column(par[0, 17:18, 0:heads])
    step = jnp.maximum(step, 0.0) + jnp.log1p(jnp.exp(-jnp.abs(step)))
    ld = -jnp.exp(column(par[0, 18:19, 0:heads])) * step + par[0, 0:hp, :]
    r_i = lax.broadcasted_iota(jnp.int32, (blk, blk), 0)
    c_i = lax.broadcasted_iota(jnp.int32, (blk, blk), 1)
    upper = jnp.where(r_i <= c_i, 1.0, 0.0).astype(F32)
    eye = jnp.where(r_i == c_i, 1.0, 0.0).astype(F32)
    lower = r_i >= c_i
    expand = jnp.where(
        lax.broadcasted_iota(jnp.int32, (hp, cw), 1) // hd == lax.broadcasted_iota(jnp.int32, (hp, cw), 0), 1.0, 0.0
    ).astype(F32)
    skips = jnp.dot(
        jnp.broadcast_to(par[0, 19:20, 0:heads], (8, heads)), expand[0:heads, :],
        precision=HIGH, preferred_element_type=F32,
    )[0:1, :]
    eye_st = jnp.where(
        lax.broadcasted_iota(jnp.int32, (st, st), 0) == lax.broadcasted_iota(jnp.int32, (st, st), 1), 1.0, 0.0
    ).astype(BF)
    cum_rs, cum_cs, st_rs, wexps = [], [], [], []
    for b in range(blocks):
        cols = slice(b * blk, (b + 1) * blk)
        cum_r = jnp.dot(ld[:, cols], upper, precision=HIGH, preferred_element_type=F32)
        st_r = step[:, cols]
        turned = bt(eye, jnp.concatenate([cum_r, st_r], axis=0), precision=HIGH)
        cum_c = turned[:, 0:hp]
        w_c = jnp.exp(cum_c[blk - 1 : blk, :] - cum_c) * turned[:, hp:]
        both = jnp.dot(
            jnp.concatenate([w_c, jnp.exp(cum_c)], axis=0), expand, precision=HIGH, preferred_element_type=F32
        )
        expd[cols, :] = both[blk:, :]
        wexps.append(both[:blk, :])
        cum_rs.append(cum_r)
        cum_cs.append(cum_c)
        st_rs.append(st_r)


    for b in range(blocks):
        for lo, hi in ((0, cw), (cw, vc)):
            total = jnp.zeros((blk, hi - lo), F32)
            for k in range(width):
                o = b * blk + raw0 - (width - 1) + k
                total = total + par[0, 24 + k : 25 + k, lo:hi] * extv[o : o + blk, lo:hi]
            conv[b * blk : (b + 1) * blk, lo:hi] = (total * jax.nn.sigmoid(total)).astype(BF)

    run = jnp.zeros((st, cw), F32)
    dec = jnp.ones((1, cw), F32)
    pres, offs = [], []
    for b in range(blocks):
        rows = slice(b * blk, (b + 1) * blk)
        key_t = bt(eye_st, conv[rows, cw : cw + st]).astype(BF)
        sv = conv[rows, 0:cw].astype(F32) * wexps[b]
        top, low = halves(sv)
        new = jnp.dot(key_t, top, preferred_element_type=F32) + jnp.dot(key_t, low, preferred_element_type=F32)
        bd = expd[(b + 1) * blk - 1 : (b + 1) * blk, :]
        pres.append(run)
        offs.append(dec)
        run = run * bd + new
        dec = dec * bd

    def inner(b):
        rows = slice(b * blk, (b + 1) * blk)
        g = bt(conv[rows, cw + st :], conv[rows, cw : cw + st])
        for h in range(cw // hd):
            gap = jnp.where(lower, cum_cs[b][:, h : h + 1] - cum_rs[b][h : h + 1, :], -jnp.inf)
            wm = g * jnp.exp(gap) * st_rs[b][h : h + 1, :]
            top, low = halves(wm)
            v = conv[rows, h * hd : (h + 1) * hd]
            scan[rows, h * hd : (h + 1) * hd] = jnp.dot(top, v, preferred_element_type=F32) + jnp.dot(
                low, v, preferred_element_type=F32
            )

    window = lax.shift_left(jnp.int32(2), tp)
    back = (
        lax.broadcasted_iota(jnp.int32, (blk, blk + raw0), 0)
        + raw0
        - lax.broadcasted_iota(jnp.int32, (blk, blk + raw0), 1)
    )
    band = jnp.where((back >= 0) & (back < window), 1.0, 0.0).astype(BF)

    def pool(b):
        rows = slice(b * blk, (b + 1) * blk)
        sums = jnp.dot(band, extp[b * blk : (b + 1) * blk + raw0, :].astype(BF), preferred_element_type=F32)
        pos = (me * n + b * blk + lax.broadcasted_iota(jnp.int32, (blk, cw), 0)).astype(F32)
        counts = jnp.minimum(pos + 1.0, window.astype(F32))
        pooled = (sums / counts - extp[b * blk + raw0 : (b + 1) * blk + raw0, :]).astype(BF)
        pbuf[pslot, rows, :] = (
            jnp.dot(pooled, mixb[0], preferred_element_type=F32) * par[0, 16:17, 0:cw]
        ).astype(BF)

    rows_of = (sbuf, pbuf)

    def rcopy(k, r, way, src=None):
        to = ({"c_": 1 - c}, {"x_": 1 - x}, {"y_": 1 - y})[way]
        src = rows_of[k].at[r] if src is None else src
        return copy(src, rows_of[k].at[r], p_ss.at[(k * T + r) * 3 + way], p_rs.at[k * T + r], **to)

    def qcopy(i):
        to = ({"c_": 1 - c}, {"x_": 1 - x}, {"x_": 1 - x, "c_": 1 - c}, {})[i]
        return copy(sq_buf.at[pslot], sq_buf.at[tp], q_ss.at[i], q_rs.at[tp], **{"y_": c, **to})

    def rows_out(k, do):
        @pl.when(moved)
        def _():
            do(rcopy(k, tp, 2, rows_of[k].at[T]))

        @pl.when(kept)
        def _():
            do(rcopy(k, tp, 1))
            do(rcopy(k, tp, 0))

    def rows_on(k, do, wait=True):
        @pl.when(kept)
        def _():
            other = 2 * x + 1 - y
            if wait:
                rcopy(k, other, 0).wait_recv()
            do(rcopy(k, other, 1))
            do(rcopy(k, other, 0))

    def rows_over(k, do, wait=True):
        @pl.when(kept)
        def _():
            for r in (2 * (1 - x) + y, 2 * (1 - x) + 1 - y):
                if wait:
                    rcopy(k, r, 0).wait_recv()
                do(rcopy(k, r, 0))

    def squares(do):
        for i in range(3):
            do(qcopy(i))

        @pl.when(moved)
        def _():
            do(qcopy(3))

    def gates():
        for r0, rows in tiles():
            d = jnp.dot(nbuf[0, rows, :], gbuf[0], preferred_element_type=F32)
            for i in range(1, S):
                d = d + jnp.dot(nbuf[i, rows, :], gbuf[i], preferred_element_type=F32)
            low = d.astype(BF)
            keep(extp, r0, low[:, 0:cw])
            gateb[r0 : r0 + mt, :] = low[0:mt, cw:]

    def pools():
        for b in range(blocks):
            pool(b)
        rows_out(1, start)

    def xpair():
        return copy(xs.at[0], xr.at[Z - 1], x_ss.at[0], x_rs.at[Z - 1], c_=1 - c)

    def xline(k):
        return copy(xs.at[1], xr.at[z], x_ss.at[k], x_rs.at[z], z_=z + k)

    def xlines(do):
        for k in reversed(range(1, Z)):
            @pl.when(z + k < Z)
            def _():
                do(xline(k))

    def put(i):
        xs[i, 0:st, :] = run
        xs[i, st:, :] = jnp.broadcast_to(dec, (xs.shape[1] - st, cw))

    put(0)
    xpair().start()

    @pl.when(kept)
    def _():
        pump(1, 3, start)

    @pl.when(moved)
    def _():
        pump(1, 2, start, when=jnp.logical_not(middle))

    for b in range(blocks // 2):
        inner(b)
    xpair().wait_recv()
    other, odec = xr[Z - 1, 0:st, :], xr[Z - 1, st : st + 1, :]
    later = c == 1
    own_s, own_d = jnp.where(later, other, 0.0), jnp.where(later, odec, 1.0)
    run = jnp.where(later, other * dec + run, run * odec + other)
    dec = dec * odec
    put(1)
    xlines(start)
    ofrom(1)

    for b in range(blocks // 2, blocks):
        inner(b)
    opass(0)

    @pl.when(moved)
    def _():
        pump(1, 3, start)

    partners(1)
    gates()
    pools()
    opass(1)
    in_s = jnp.zeros((st, cw), F32)
    for p in range(Z - 1):
        @pl.when(z > p)
        def _():
            copy(xs.at[1], xr.at[p], x_ss.at[1], x_rs.at[p], c_=1 - c).wait_recv()

        in_s = jnp.where(z > p, in_s * xr[p, st : st + 1, :] + xr[p, 0:st, :], in_s)
    in_s = in_s * own_d + own_s

    for b in range(blocks):
        rows = slice(b * blk, (b + 1) * blk)
        top, low = halves(pres[b] + offs[b] * in_s)
        rd = conv[rows, cw + st :]
        carried = jnp.dot(rd, top, preferred_element_type=F32) + jnp.dot(rd, low, preferred_element_type=F32)
        out_b = scan[rows, :] + carried * expd[rows, :] + skips * conv[rows, 0:cw].astype(F32)
        gt = gateb[rows, :].astype(F32)
        gated = out_b * (gt * jax.nn.sigmoid(gt))
        sq_buf[pslot, :, rows] = bt(jnp.ones((8, cw), F32), gated * gated, precision=HIGH)
        sbuf[pslot, rows, :] = (gated * par[0, 16:17, cw : 2 * cw]).astype(BF)

    rows_out(0, start)
    squares(start)
    olate()
    oend(0, 0)
    oend(1, 0)
    rows_on(1, start)
    ofar(0, start)
    oend(1, 1)
    oend(0, 1)
    rows_on(0, start)
    ofar(1, start)
    rows_over(1, start)
    rows_over(0, start)
    @pl.when(moved)
    def _():
        for k in range(2):
            for r in range(T):
                rcopy(k, r, 0).wait_recv()

    for r in range(T):
        @pl.when((tp != r) | moved)
        def _():
            copy(sq_buf.at[r], sq_buf.at[r], q_ss.at[0], q_rs.at[r], c_=1 - c).wait_recv()

    for q in range(T):
        i = (1 - y) * T + q
        copy(obuf.at[i], obuf.at[i], o_ss.at[0], o_rs.at[i], y_=1 - y).wait_recv()

    sq = sum(sq_buf[r] for r in range(T))
    rs_row = lax.rsqrt(sq / (cw * T) + EPSILON)
    rs_cols = [bt(eye, rs_row[:, b * blk : (b + 1) * blk], precision=HIGH)[:, 0:1] for b in range(blocks)]
    for r0 in range(0, n, mt):
        rows = slice(r0, r0 + mt)
        rs = jnp.concatenate(rs_cols[r0 // blk : (r0 + mt) // blk], axis=0)
        for j in range(2):
            p = jnp.dot(pbuf[0, rows, :], obuf[j * T, 0:cw, :], preferred_element_type=F32)
            s = jnp.dot(sbuf[0, rows, :], obuf[j * T, cw:, :], preferred_element_type=F32)
            for q in range(1, T):
                p = p + jnp.dot(pbuf[q, rows, :], obuf[j * T + q, 0:cw, :], preferred_element_type=F32)
                s = s + jnp.dot(sbuf[q, rows, :], obuf[j * T + q, cw:, :], preferred_element_type=F32)
            out[rows, j * oc : (j + 1) * oc] = (p + rs * s).astype(out.dtype)

    for k in range(2):
        source(k, done)
        for d in range(1, Z):
            pump(k, d, done, wait=False)
        rows_out(k, done)
        rows_on(k, done, wait=False)
        rows_over(k, done, wait=False)
    oall(done)
    squares(done)
    acopy(1).wait_send()
    acopy(2).wait_send()

    @pl.when(moved)
    def _():
        acopy(0).wait_send()
        for i in range(4):
            swap(i).wait_send()
        aforward(0).wait_send()

    @pl.when(kept)
    def _():
        aforward(1).wait_send()

    @pl.when(jnp.logical_not(hub))
    def _():
        ohub().wait_send()

    xpair().wait_send()
    xlines(done)

    hsends(done)


def fits(S, T, shapes):
    n, da = shapes[0]
    kd, cw = shapes[2]
    st = shapes[5][1]
    oc = shapes[18][1]
    heads = shapes[7][1]
    taps = shapes[10][0]
    return (
        T == 4 == POOL_GROUPS and S == 2 * T and st == SSM_STATE and taps <= 8 and heads <= 8
        and cw == heads * SSM_STATE and n % 256 == 0 and n % SCAN_BLOCK == 0 and n >= 2 * cw
        and oc % 128 == 0 and kd % 128 == 0 and da % kd == 0 and da * T == kd * S and kd <= cw + 2 * st
        and cw % 128 == 0 and oc * 2 == da
    )


def fused(
    S, T, activations, norm_gain, pool_weight, gate_weight, value_weight, key_weight, read_weight,
    step_weight, pool_mix, pool_scale, taps_value, taps_key, taps_read, step_bias, decay_log,
    decay_extra, skip_scale, state_gain, out_pool_weight, out_state_weight,
):
    n, da = activations.shape
    kd, cw = pool_weight.shape
    st = key_weight.shape[1]
    oc = out_pool_weight.shape[1]
    hp = 16
    args = (
        activations, norm_gain[None, :], pool_weight, gate_weight, value_weight, key_weight.T, read_weight.T,
        step_weight.T, pool_mix, pool_scale[None, :], taps_value, taps_key, taps_read, step_bias[None, :], decay_log[None, :],
        decay_extra.T, skip_scale[None, :], state_gain[None, :],
        out_pool_weight, out_state_weight,
    )
    vc = cw + 2 * st
    V = pltpu.VMEM
    D = pltpu.SemaphoreType.DMA
    scratch = [
        V((S + 1, kd + hp, vc), BF), V((S + 1, kd, 2 * cw), BF), V((2 * T + 3, 2 * cw, oc), BF),
        V((T + 1, n + 16, da), BF), V((2, cw, cw), BF), V((2, 32, n), F32),
        V((S, n + 16, kd), BF), V((n + 16, vc), F32), V((n + 16, cw), F32), V((n, cw), BF), V((n, vc), BF),
        V((T, 16, da), BF), V((n, cw), F32),
        V((2, st + 8, cw), F32), V((S // 2, st + 8, cw), F32),
        V((T + 1, 8, n), F32), V((T + 1, n, cw), BF), V((T + 1, n, cw), BF), V((n, cw), F32),
        D((10 * S,)), D((2 * S,)), D((27,)), D((2 * T + 3,)), D((5,)), D((T,)), D((4,)), D((2,)),
        D((4,)), D((T,)), D((S // 2,)), D((S // 2,)), D((4,)), D((T,)), D((6 * T,)), D((2 * T,)),
    ]
    return pl.pallas_call(
        functools.partial(mixer_kernel, S, T),
        out_shape=jax.ShapeDtypeStruct((n, da), BF),
        in_specs=[pl.BlockSpec(memory_space=pltpu.VMEM)] * len(args),
        out_specs=pl.BlockSpec(memory_space=pltpu.VMEM),
        scratch_shapes=scratch,
        compiler_params=pltpu.CompilerParams(
            collective_id=0, has_side_effects=True, vmem_limit_bytes=60 * 1024 * 1024
        ),
    )(*args)


def solution(mesh):
    placed = (
        P("sp", "tp"),
        P("tp"),
        P("sp", "tp"),
        P("sp", "tp"),
        P("sp", "tp"),
        P("sp", "tp"),
        P("sp", "tp"),
        P("sp", "tp"),
        P("tp", None, None),
        P("tp"),
        P(None, "tp"),
        P(None, "tp"),
        P(None, "tp"),
        P("tp"),
        P("tp"),
        P("sp", "tp"),
        P("tp"),
        P("tp"),
        P("tp", "sp"),
        P("tp", "sp"),
    )
    S, T = mesh.shape["sp"], mesh.shape["tp"]

    def chosen(*args):
        if fits(S, T, [a.shape for a in args]):
            return fused(S, T, *args)
        return local(*args)

    return jax.shard_map(
        chosen, mesh=mesh, in_specs=placed, out_specs=P("sp", "tp"), check_vma=False
    )
```

```python
import functools

import jax
import jax.numpy as jnp
from jax import lax
from jax.experimental import pallas as pl
from jax.experimental.pallas import tpu as pltpu
from jax.sharding import PartitionSpec as P

SSM_STATE = 64
POOL_GROUPS = 4
SCAN_BLOCK = 128
MIX_W = 1024


EPSILON = 1e-06
HIGH = lax.Precision.HIGHEST


def shifted(value, axis, steps):
    count = lax.axis_size(axis)
    leading, last = (max(0, -steps), min(count, count - steps))
    return lax.ppermute(value, axis, [(source, source + steps) for source in range(leading, last)])


def carried_in(part, axis, combine, identity):
    place = lax.axis_index(axis)
    gathered = jax.tree.map(lambda a: lax.all_gather(a, axis), part)
    state = jax.tree.map(lambda a, e: jnp.zeros_like(a) + jnp.asarray(e, a.dtype), part, identity)

    def one(step, state):
        return combine(
            state, jax.tree.map(lambda a: lax.dynamic_index_in_dim(a, step, 0, False), gathered)
        )

    return lax.fori_loop(0, place, one, state)


def backward_kernel(extended, taps):
    width = taps.shape[0]
    length = extended.shape[0] - (width - 1)
    widened_rows = extended.astype(jnp.float32)
    total = jnp.zeros((length, extended.shape[1]), jnp.float32)
    for offset in range(width):
        total = total + taps[offset][None, :] * widened_rows[offset : offset + length]
    return jax.nn.silu(total).astype(jnp.bfloat16)


def combine_states(preceding_token, later):
    return (preceding_token[0] * later[0], preceding_token[1] * later[0][:, None, None] + later[1])


def local(
    activations,
    norm_gain,
    pool_weight,
    gate_weight,
    value_weight,
    key_weight,
    read_weight,
    step_weight,
    pool_mix,
    pool_scale,
    taps_value,
    taps_key,
    taps_read,
    step_bias,
    decay_log,
    decay_extra,
    skip_scale,
    state_gain,
    out_pool_weight,
    out_state_weight,
):
    length = activations.shape[0]
    cluster_span = pool_weight.shape[1]
    local_mix = gate_weight.shape[1]
    local_state = key_weight.shape[1]
    local_heads = step_weight.shape[1]
    joined = jnp.concatenate(
        [pool_weight, gate_weight, value_weight, key_weight, read_weight, step_weight], axis=1
    )
    in_weight = lax.all_gather(joined, "sp", axis=0, tiled=True)
    whole, gains = (
        lax.all_gather(activations, "tp", axis=1, tiled=True),
        lax.all_gather(norm_gain, "tp", axis=0, tiled=True),
    )
    widened_rows = whole.astype(jnp.float32)
    normed = (
        widened_rows
        * lax.rsqrt(jnp.mean(widened_rows * widened_rows, axis=-1, keepdims=True) + EPSILON)
        * gains.astype(jnp.float32)
    ).astype(jnp.bfloat16)
    projected = jnp.dot(normed, in_weight, preferred_element_type=jnp.float32)
    column = 0
    pool_in = projected[:, column : column + cluster_span].astype(jnp.bfloat16)
    column = column + cluster_span
    gate_in = projected[:, column : column + local_mix].astype(jnp.bfloat16)
    column = column + local_mix
    raw_value = projected[:, column : column + local_mix].astype(jnp.bfloat16)
    column = column + local_mix
    raw_key = projected[:, column : column + local_state].astype(jnp.bfloat16)
    column = column + local_state
    raw_read = projected[:, column : column + local_state].astype(jnp.bfloat16)
    column = column + local_state
    step_raw = projected[:, column : column + local_heads]
    raw_joined = jnp.concatenate([raw_value, raw_key, raw_read], axis=1)
    reach = 2**POOL_GROUPS - 1
    width = taps_value.shape[0]
    prior_pool, prior_joined = shifted(
        (pool_in[length - reach :], raw_joined[length - width + 1 :]), "sp", 1
    )
    group = lax.axis_index("tp")
    running = jnp.concatenate([prior_pool, pool_in], axis=0).astype(jnp.float32)
    levels = []
    for level in range(POOL_GROUPS):
        stride = 2**level
        running = running[stride:] + running[:-stride]
        levels.append(running[running.shape[0] - length :])
    window_sum = lax.dynamic_index_in_dim(jnp.stack(levels), group, 0, keepdims=False)
    window = jnp.exp2((group + 1).astype(jnp.float32))
    position = (lax.axis_index("sp") * length + jnp.arange(length, dtype=jnp.int32)).astype(
        jnp.float32
    )
    counts = jnp.minimum(position + 1.0, window)
    pooled = (window_sum / counts[:, None] - pool_in.astype(jnp.float32)).astype(jnp.bfloat16)
    pool_out = (
        jnp.dot(pooled, pool_mix[0], preferred_element_type=jnp.float32) * pool_scale
    ).astype(jnp.bfloat16)
    all_taps = jnp.concatenate([taps_value, taps_key, taps_read], axis=1)
    convolved = backward_kernel(jnp.concatenate([prior_joined, raw_joined], axis=0), all_taps)
    head_value = convolved[:, :local_mix]
    key_vectors = convolved[:, local_mix : local_mix + local_state]
    read_vectors = convolved[:, local_mix + local_state :]
    head_dim = local_mix // local_heads
    groups_here = local_state // SSM_STATE
    repeat = local_heads // groups_here
    blocks = length // SCAN_BLOCK
    step_size = jax.nn.softplus(step_raw + step_bias)
    log_decay = -jnp.exp(decay_log) * step_size + decay_extra
    value_heads = head_value.astype(jnp.float32).reshape(length, local_heads, head_dim)
    value_blocks = value_heads.reshape(blocks, SCAN_BLOCK, local_heads, head_dim)
    key_blocks = jnp.repeat(
        key_vectors.astype(jnp.float32).reshape(length, groups_here, SSM_STATE), repeat, axis=1
    ).reshape(blocks, SCAN_BLOCK, local_heads, SSM_STATE)
    read_blocks = jnp.repeat(
        read_vectors.astype(jnp.float32).reshape(length, groups_here, SSM_STATE), repeat, axis=1
    ).reshape(blocks, SCAN_BLOCK, local_heads, SSM_STATE)
    step_blocks = step_size.reshape(blocks, SCAN_BLOCK, local_heads)
    running_decay = jnp.cumsum(log_decay.reshape(blocks, SCAN_BLOCK, local_heads), axis=1)
    lower = jnp.arange(SCAN_BLOCK)[:, None] >= jnp.arange(SCAN_BLOCK)[None, :]
    gaps = jnp.where(
        lower[None, :, :, None],
        running_decay[:, :, None, :] - running_decay[:, None, :, :],
        -jnp.inf,
    )
    weights = jnp.einsum("blhn,bshn->blsh", read_blocks, key_blocks, precision=HIGH) * jnp.exp(gaps)
    scaled_value = value_blocks * step_blocks[..., None]
    inner = jnp.einsum("blsh,bshp->blhp", weights, scaled_value, precision=HIGH)
    block_ends = running_decay[:, -1, :]
    trailing = jnp.exp(block_ends[:, None, :] - running_decay)
    fresh = jnp.einsum("bshn,bsh,bshp->bhpn", key_blocks, trailing, scaled_value, precision=HIGH)

    def advance(carry, inputs):
        block_decay, block_state = inputs
        return (carry * block_decay[:, None, None] + block_state, carry)

    local_total, prefix = lax.scan(
        advance,
        jnp.zeros((local_heads, head_dim, SSM_STATE), jnp.float32),
        (jnp.exp(block_ends), fresh),
    )
    offsets = jnp.cumsum(block_ends, axis=0) - block_ends
    device_decay = jnp.exp(offsets[-1] + block_ends[-1])
    incoming_decay, incoming = carried_in(
        (device_decay, local_total),
        "sp",
        combine_states,
        (jnp.ones_like(device_decay), jnp.zeros_like(local_total)),
    )
    from_device = running_decay + offsets[:, None, :]
    local_off = (
        jnp.einsum("blhn,bhpn->blhp", read_blocks, prefix, precision=HIGH)
        * jnp.exp(running_decay)[..., None]
    )
    far_off = (
        jnp.einsum("blhn,hpn->blhp", read_blocks, incoming, precision=HIGH)
        * jnp.exp(from_device)[..., None]
    )
    scan_out = (inner + local_off + far_off).reshape(length, local_heads, head_dim) + skip_scale[
        None, :, None
    ] * value_heads
    gated = scan_out.reshape(length, local_mix) * jax.nn.silu(gate_in.astype(jnp.float32))
    gate_squares = lax.psum(jnp.sum(gated * gated, axis=-1), "tp")
    state_out = (gated * lax.rsqrt(gate_squares / MIX_W + EPSILON)[:, None] * state_gain).astype(
        jnp.bfloat16
    )
    branch_rows = jnp.concatenate([pool_out, state_out], axis=1)
    out_weight = jnp.concatenate([out_pool_weight, out_state_weight], axis=0)
    terms = jnp.dot(
        branch_rows,
        lax.all_gather(out_weight, "sp", axis=1, tiled=True),
        preferred_element_type=jnp.float32,
    )
    result = lax.psum_scatter(terms, "tp", scatter_dimension=1, tiled=True)
    return result.astype(jnp.bfloat16)


BF = jnp.bfloat16
F32 = jnp.float32
MESH = pl.DeviceIdType.MESH


def flip(index, mask):
    bit = 1
    while bit <= mask:
        if mask & bit:
            index = index + bit - 2 * bit * lax.rem(lax.div(index, bit), 2)
        bit *= 2
    return index


def bt(a, b, **kw):
    return lax.dot_general(a, b, (((1,), (1,)), ((), ())), preferred_element_type=F32, **kw)


def halves(x):
    top = x.astype(BF)
    return top, (x - top.astype(F32)).astype(BF)


TWIN = 2


def mixer_kernel(
    S, T,
    act, gain, pool_w, gate_w, value_w, key_w, read_w, step_t, mix, scale, taps_v, taps_k, taps_r,
    bias, dlog, extra_t, skip, sgain, opool, ostate,
    out,
    vbuf, gbuf, obuf, abuf, mixb, par, nbuf, extv, extp, gateb, conv, hbuf, scan, xs, xr,
    sq_buf, pbuf, sbuf, expd,
    b_ss, b_rs, o_ss, o_rs, a_ss, a_rs, t_ss, t_rs, h_ss, h_rs, x_ss, x_rs, q_ss, q_rs, p_ss, p_rs,
):
    n, da = act.shape
    kd, cw = pool_w.shape
    st = key_w.shape[0]
    heads = step_t.shape[0]
    hp = vbuf.shape[1] - kd
    vc = cw + 2 * st
    oc = opool.shape[1]
    blk = SCAN_BLOCK
    blocks = n // blk
    hd = SSM_STATE
    Z = S // 2
    sp, tq = lax.axis_index("sp"), lax.axis_index("tp")
    z, y = lax.div(sp, 2), lax.rem(sp, 2)
    x, c = lax.div(tq, 2), lax.rem(tq, 2)
    me, tp = 2 * z + c, 2 * x + y
    off = lax.rem(y + c, 2)
    moved, kept = off == 1, off == 0
    slot = me + off * (S - me)
    aslot = tq + off * (T - tq)
    pslot = tp + off * (T - tp)
    hubs = (tq == z, 2 * (1 - x) + c == z)
    hub = hubs[0] | hubs[1]
    turn = lax.rem(y + c, 2)
    oslot = jnp.where(hubs[0], y * T + tq, jnp.where(hubs[1], 2 * T + 1 + turn, 2 * T))

    def dev(z_=z, y_=y, x_=x, c_=c):
        return {"sp": 2 * z_ + y_, "tp": 2 * x_ + c_}

    def copy(src, dst, ss, rs, **to):
        return pltpu.make_async_remote_copy(
            src_ref=src, dst_ref=dst, send_sem=ss, recv_sem=rs, device_id=dev(**to), device_id_type=MESH
        )

    barrier = pltpu.get_barrier_semaphore()

    def greet(**to):
        pl.semaphore_signal(barrier, inc=1, device_id=dev(**to), device_id_type=MESH)

    for dz in range(Z):
        for k in range(8):
            if dz or k:
                greet(
                    z_=lax.rem(z + dz, Z), y_=1 - y if k & 4 else y, x_=1 - x if k & 2 else x,
                    c_=1 - c if k & 1 else c,
                )

    eye_kd = jnp.where(
        lax.broadcasted_iota(jnp.int32, (kd, kd), 0) == lax.broadcasted_iota(jnp.int32, (kd, kd), 1), 1.0, 0.0
    ).astype(BF)
    pick = jnp.where(
        lax.broadcasted_iota(jnp.int32, (hp, heads), 0) == lax.broadcasted_iota(jnp.int32, (hp, heads), 1), 1.0, 0.0
    ).astype(F32)
    vbuf[slot, 0:kd, 0:cw] = value_w[...]
    vbuf[slot, 0:kd, cw:] = bt(eye_kd, jnp.concatenate([key_w[...], read_w[...]], axis=0)).astype(BF)
    vbuf[slot, kd:, :] = jnp.zeros((hp, vc), BF)
    vbuf[slot, kd:, 0:kd] = jnp.dot(pick.astype(BF), step_t[...], preferred_element_type=F32).astype(BF)
    abuf[aslot, 0:n, :] = act[...]
    for i in range(gain.shape[0]):
        g = jnp.broadcast_to(gain[i : i + 1, :].astype(F32), (16, gain.shape[1]))
        abuf[aslot, n : n + 16, i * gain.shape[1] : (i + 1) * gain.shape[1]] = g.astype(BF)

    gbuf[slot, :, 0:cw] = pool_w[...]
    gbuf[slot, :, cw:] = gate_w[...]
    obuf[oslot, 0:cw, :] = opool[...]
    obuf[oslot, cw:, :] = ostate[...]
    mixb[off] = mix[0]
    par[off] = jnp.zeros(par.shape[1:], F32)
    par[off, 0:heads, :] = extra_t[...]
    par[off, 16:17, 0:cw] = scale[...]
    par[off, 16:17, cw : 2 * cw] = sgain[...]
    par[off, 17:18, 0:heads] = bias[...]
    par[off, 18:19, 0:heads] = dlog[...]
    par[off, 19:20, 0:heads] = skip[...]
    width = taps_v.shape[0]
    par[off, 24 : 24 + width, 0:cw] = taps_v[...]
    par[off, 24 : 24 + width, cw : cw + st] = taps_k[...]
    par[off, 24 : 24 + width, cw + st : vc] = taps_r[...]
    pl.semaphore_wait(barrier, S * T - 1)

    raw0 = hbuf.shape[1]
    own_halo = (y == 0) & (c == 1)

    @pl.when(own_halo)
    def _():
        hbuf[tq] = act[n - raw0 :, :]

    @pl.when(me == 0)
    def _():
        hbuf[...] = jnp.zeros(hbuf.shape, BF)

    middle = (z == 1) | (z == Z - 2)
    streams = (vbuf, gbuf)

    def bcopy(k, i, way):
        to = ({"c_": 1 - c}, {"z_": z + 1}, {"z_": z - 1}, {"z_": z + 2}, {"z_": z - 2})[way]
        ref = streams[k].at[i]
        return copy(ref, ref, b_ss.at[(k * S + i) * 5 + way], b_rs.at[k * S + i], **to)

    def arrived(k, i):
        bcopy(k, i, 0).wait_recv()

    def source(k, do):
        ways = [(1, z < Z - 1), (2, z > 0)]
        if k:
            ways = [(3, moved & (z == 0)), (4, moved & (z == Z - 1))] + ways
        for way, when in ways:
            @pl.when(when)
            def _():
                do(bcopy(k, me, way))

        do(bcopy(k, me, 0))

    def start(d):
        d.start()

    def done(d):
        d.wait_send()

    def pump(k, d, do, wait=True, when=True):
        right, left = z < Z - 1, z > 0
        if k and d == 1:
            right, left = right & (kept | (z > 1)), left & (kept | (z < Z - 2))

        @pl.when((z >= d) & when)
        def _():
            i = 2 * (z - d) + c
            if wait:
                arrived(k, i)

            @pl.when(right)
            def _():
                do(bcopy(k, i, 1))

            do(bcopy(k, i, 0))

        @pl.when((z + d < Z) & when)
        def _():
            i = 2 * (z + d) + c
            if wait:
                arrived(k, i)

            @pl.when(left)
            def _():
                do(bcopy(k, i, 2))

            do(bcopy(k, i, 0))

    def partners(k):
        for p in range(Z):
            arrived(k, 2 * p + 1 - c)

    def swap(i):
        src, dst, rs = (
            (vbuf.at[S], vbuf.at[sp], b_rs.at[sp]),
            (par.at[1], par.at[0], t_rs.at[0]),
            (gbuf.at[S], gbuf.at[sp], b_rs.at[S + sp]),
            (mixb.at[1], mixb.at[0], t_rs.at[1]),
        )[i]
        return copy(src, dst, t_ss.at[i], rs, y_=c, c_=y)

    def acopy(way):
        to = ({"c_": y}, {"x_": 1 - x, "c_": y}, {"y_": 1 - y, "c_": y})[way]
        return copy(abuf.at[aslot], abuf.at[tq], a_ss.at[way], a_rs.at[tq], **to)

    def aforward(i):
        t, to = ((2 * x + 1 - c, {"x_": 1 - x}), (2 * (1 - x) + c, {"y_": 1 - y}))[i]
        return copy(abuf.at[t], abuf.at[t], a_ss.at[3 + i], a_rs.at[t], **to)

    def agot(t):
        copy(abuf.at[t], abuf.at[t], a_ss.at[0], a_rs.at[t], x_=1 - x).wait_recv()

    def hcopy(k):
        return copy(
            abuf.at[aslot, pl.ds(n - raw0, raw0)], hbuf.at[tq], h_ss.at[k], h_rs.at[tq],
            z_=z + y, y_=k // 2, x_=k % 2, c_=1 - y,
        )

    def hsends(do):
        @pl.when(sp < S - 1)
        def _():
            for k in range(4):
                @pl.when(jnp.logical_not(own_halo & (y == k // 2) & (x == k % 2)))
                def _():
                    do(hcopy(k))

    def hgot():
        @pl.when(me > 0)
        def _():
            for t in range(T):
                @pl.when(jnp.logical_not(own_halo & (tq == t)))
                def _():
                    copy(hbuf.at[t], hbuf.at[t], h_ss.at[0], h_rs.at[t], x_=1 - x).wait_recv()

    def oquarter(j):
        return 2 * x + (y if j == 0 else 1 - y)

    def oslots(line, j):
        return 2 * T + 1 + j if line else y * T + oquarter(j)

    def ohub():
        home = lax.div(z, 2) == x
        dst = jnp.where(home, y * T + tq, 2 * T + 1 + turn)
        return copy(obuf.at[2 * T], obuf.at[dst], o_ss.at[0], o_rs.at[dst], c_=1 - c)

    def ocopy(line, j, way, final=False):
        to = (
            {"z_": z + 1}, {"z_": z - 1}, {"z_": z + 2}, {"z_": z - 2},
            {"x_": 1 - x} if line else {"y_": 1 - y},
        )[way]
        if final and line:
            to = {"x_": 1 - x, **to}
        i = oslots(line, j)
        dst = i if way < 4 and not final else y * T + oquarter(j)
        return copy(obuf.at[i], obuf.at[dst], o_ss.at[1 + (2 * line + j) * 6 + way], o_rs.at[dst], **to)

    def owait(line, j):
        i = oslots(line, j)
        copy(obuf.at[i], obuf.at[i], o_ss.at[0], o_rs.at[i], x_=1 - x).wait_recv()

    def across(line, j, do):
        if not line:
            do(ocopy(line, j, 4))

    def over(line, j, do):
        if line:
            do(ocopy(line, j, 4))

    def osend(line, j, do):
        for way, final, when in (
            (2, False, z == 0), (3, False, z == Z - 1), (0, False, z == 1), (1, True, z == 1),
            (1, False, z == Z - 2), (0, True, z == Z - 2),
        ):
            @pl.when(when)
            def _():
                do(ocopy(line, j, way, final))

    def center(line):
        return 2 * (1 - x) + c if line else tq

    def relays(line):
        h = center(line)
        return ((z == Z - 2) & (h < 2)) | ((z == 1) & (h > 1))

    def orelay(line, j, do):
        h = center(line)
        for way, when in ((0, h < 2), (1, h > 1), (1, h == 0), (0, h == T - 1)):
            @pl.when(when)
            def _():
                do(ocopy(line, j, way, True))

    def ofrom(j, when=True):
        for line in range(2):
            @pl.when(hubs[line] & when)
            def _():
                osend(line, j, start)

    def ocross():
        for line in range(2):
            @pl.when(hubs[line])
            def _():
                for j in range(2):
                    @pl.when(turn != j)
                    def _():
                        owait(line, j)

                    over(line, j, start)
                    across(line, j, start)

    def opass(j, when=True):
        for line in range(2):
            @pl.when(relays(line) & when)
            def _():
                owait(line, j)
                orelay(line, j, start)
                over(line, j, start)

                @pl.when(kept)
                def _():
                    across(line, j, start)

    def olate():
        for line in range(2):
            @pl.when(relays(line) & moved)
            def _():
                for j in range(2):
                    across(line, j, start)

    def oend(j):
        @pl.when(jnp.logical_not(hubs[0] | relays(0)))
        def _():
            owait(0, j)

            @pl.when(jnp.logical_not(last & (j < TWIN)))
            def _():
                across(0, j, start)

    last = ((z == Z - 1) & (x == 0)) | ((z == 0) & (x == 1))

    def otwin(j, do, wait=True):
        @pl.when(relays(0))
        def _():
            i = (1 - y) * T + 2 * x + (1 - y if j == 0 else y)
            d = copy(obuf.at[i], obuf.at[i], o_ss.at[27 + j], o_rs.at[i], z_=z + 1 - 2 * x)
            if wait:
                d.wait_recv()
            do(d)

    def ofar(j, do, wait=True):
        i = y * T + 2 * (1 - x) + (y if j == 0 else 1 - y)
        d = copy(obuf.at[i], obuf.at[i], o_ss.at[25 + j], o_rs.at[i], y_=1 - y)
        if wait:
            d.wait_recv()
        do(d)

    def oall(do):
        for j in range(2):
            ofar(j, do, False)

        for line in range(2):
            for j in range(2):
                @pl.when(hubs[line])
                def _():
                    osend(line, j, do)

                @pl.when(relays(line))
                def _():
                    orelay(line, j, do)

                @pl.when(hubs[line] | relays(line))
                def _():
                    over(line, j, do)

                @pl.when(jnp.logical_not(last & (j < TWIN)))
                def _():
                    across(line, j, do)

        for j in range(TWIN):
            otwin(j, do, False)

    @pl.when(moved)
    def _():
        swap(0).start()

    acopy(1).start()
    hsends(start)

    @pl.when(moved)
    def _():
        acopy(2).start()
        acopy(0).start()
        swap(2).start()
        swap(1).start()

        @pl.when(jnp.logical_not(hub))
        def _():
            ohub().start()

    @pl.when(moved)
    def _():
        arrived(0, me)

    source(0, start)

    @pl.when(kept)
    def _():
        source(1, start)

    pump(0, 1, start)

    @pl.when(kept)
    def _():
        acopy(2).start()
        agot(2 * (1 - x) + c)
        aforward(1).start()

        @pl.when(jnp.logical_not(hub))
        def _():
            ohub().start()

    @pl.when(moved)
    def _():
        agot(2 * x + 1 - c)
        aforward(0).start()

    pump(0, 2, start)

    pump(0, 3, start)

    @pl.when(moved)
    def _():
        swap(3).start()
        arrived(1, me)
        source(1, start)

    @pl.when(kept)
    def _():
        pump(1, 1, start)

    partners(0)
    @pl.when(moved)
    def _():
        swap(1).wait_recv()

    def column(row):
        return bt(pick, jnp.broadcast_to(row, (8, heads)), precision=HIGH)[:, 0:1]

    bias_c = column(par[0, 17:18, 0:heads])
    rate_c = -jnp.exp(column(par[0, 18:19, 0:heads]))
    r_i = lax.broadcasted_iota(jnp.int32, (blk, blk), 0)
    c_i = lax.broadcasted_iota(jnp.int32, (blk, blk), 1)
    eye = jnp.where(r_i == c_i, 1.0, 0.0).astype(F32)
    lower = r_i >= c_i
    expand = jnp.where(
        lax.broadcasted_iota(jnp.int32, (hp, cw), 1) // hd == lax.broadcasted_iota(jnp.int32, (hp, cw), 0), 1.0, 0.0
    ).astype(F32)
    skips = jnp.dot(
        jnp.broadcast_to(par[0, 19:20, 0:heads], (8, heads)), expand[0:heads, :],
        precision=HIGH, preferred_element_type=F32,
    )[0:1, :]
    eye_st = jnp.where(
        lax.broadcasted_iota(jnp.int32, (st, st), 0) == lax.broadcasted_iota(jnp.int32, (st, st), 1), 1.0, 0.0
    ).astype(BF)

    def thirds(v):
        top = v.astype(BF)
        rest = v - top.astype(F32)
        mid = rest.astype(BF)
        return jnp.concatenate([top, mid, (rest - mid.astype(F32)).astype(BF)], axis=1)

    upper = jnp.concatenate([jnp.where(r_i <= c_i, 1.0, 0.0).astype(BF)] * 3, axis=0)
    row = lax.rem(lax.broadcasted_iota(jnp.int32, (3 * blocks * hp, blocks * cw), 0), blocks * hp)
    col = lax.broadcasted_iota(jnp.int32, (3 * blocks * hp, blocks * cw), 1)
    spread = jnp.where(row == (col // cw) * hp + lax.rem(col, cw) // hd, 1.0, 0.0).astype(BF)


    @pl.when(kept)
    def _():
        agot(2 * x + 1 - c)

    @pl.when(moved)
    def _():
        agot(2 * x + c)
        agot(2 * (1 - x) + c)

    agot(2 * (1 - x) + 1 - c)
    hgot()

    ocross()
    ofrom(0, middle & moved)
    per = da // kd
    rt = 64

    def norm_rows(parts, r):
        tot = sum(jnp.sum(p * p, axis=-1, keepdims=True) for p in parts)
        rs = lax.rsqrt(tot / (da * T) + EPSILON)
        for t in range(T):
            g = abuf[t, n : n + 1, :].astype(F32)
            v = (parts[t] * rs * g).astype(BF)
            for j in range(per):
                nbuf[t * per + j, r, :] = v[:, j * kd : (j + 1) * kd]

    def norm_tile(i, _):
        r = pl.ds(pl.multiple_of(i * rt, rt), rt)
        norm_rows([abuf[t, r, :].astype(F32) for t in range(T)], r)
        return 0

    lax.fori_loop(0, n // rt, norm_tile, 0)
    norm_rows([hbuf[t].astype(F32) for t in range(T)], pl.ds(n, raw0))
    @pl.when(moved)
    def _():
        pump(1, 1, start)


    mt = 256

    def tiles():
        for r0 in range(0, n, mt):
            yield r0, slice(r0, r0 + mt + raw0 if r0 + mt == n else r0 + mt)

    def keep(ref, r0, low):
        ref[raw0 + r0 : raw0 + r0 + mt, :] = low[0:mt, :].astype(F32)
        if low.shape[0] > mt:
            ref[0:raw0, :] = low[mt:, :].astype(F32)

    for r0, rows in tiles():
        d = jnp.dot(nbuf[0, rows, :], vbuf[0, 0:kd, :], preferred_element_type=F32)
        for i in range(1, S):
            d = d + jnp.dot(nbuf[i, rows, :], vbuf[i, 0:kd, :], preferred_element_type=F32)
        keep(extv, r0, d.astype(BF))

    sacc = bt(vbuf[0, kd:, 0:kd], nbuf[0, 0:n, :])
    for i in range(1, S):
        sacc = sacc + bt(vbuf[i, kd:, 0:kd], nbuf[i, 0:n, :])
    @pl.when(kept)
    def _():
        pump(1, 2, start)

    @pl.when(moved)
    def _():
        pump(1, 2, start, when=middle)

    ofrom(0, jnp.logical_not(middle & moved))

    step = sacc + bias_c
    step = jnp.maximum(step, 0.0) + jnp.log1p(jnp.exp(-jnp.abs(step)))
    ld = rate_c * step + par[0, 0:hp, :]

    def stacked(v):
        return jnp.concatenate([v[:, b * blk : (b + 1) * blk] for b in range(blocks)], axis=0)

    cum_r = jnp.dot(thirds(stacked(ld)), upper, preferred_element_type=F32)
    st_r = stacked(step)
    cum_c = cum_r.T
    grown = jnp.exp(cum_c)
    left = jnp.exp(cum_c[blk - 1 : blk, :] - cum_c) * st_r.T
    both = jnp.dot(thirds(jnp.concatenate([left, grown], axis=0)), spread, preferred_element_type=F32)
    cum_rs, cum_cs, st_rs, wexps = [], [], [], []
    for b in range(blocks):
        expd[b * blk : (b + 1) * blk, :] = both[blk:, b * cw : (b + 1) * cw]
        wexps.append(both[:blk, b * cw : (b + 1) * cw])
        cum_rs.append(cum_r[b * hp : (b + 1) * hp, :])
        cum_cs.append(cum_c[:, b * hp : (b + 1) * hp])
        st_rs.append(st_r[b * hp : (b + 1) * hp, :])


    for b in range(blocks):
        for lo, hi in ((0, cw), (cw, vc)):
            total = jnp.zeros((blk, hi - lo), F32)
            for k in range(width):
                o = b * blk + raw0 - (width - 1) + k
                total = total + par[0, 24 + k : 25 + k, lo:hi] * extv[o : o + blk, lo:hi]
            conv[b * blk : (b + 1) * blk, lo:hi] = (total * jax.nn.sigmoid(total)).astype(BF)

    run = jnp.zeros((st, cw), F32)
    dec = jnp.ones((1, cw), F32)
    pres, offs = [], []
    for b in range(blocks):
        rows = slice(b * blk, (b + 1) * blk)
        key_t = bt(eye_st, conv[rows, cw : cw + st]).astype(BF)
        sv = conv[rows, 0:cw].astype(F32) * wexps[b]
        top, low = halves(sv)
        new = jnp.dot(key_t, top, preferred_element_type=F32) + jnp.dot(key_t, low, preferred_element_type=F32)
        bd = expd[(b + 1) * blk - 1 : (b + 1) * blk, :]
        pres.append(run)
        offs.append(dec)
        run = run * bd + new
        dec = dec * bd

    def inner(b):
        rows = slice(b * blk, (b + 1) * blk)
        g = bt(conv[rows, cw + st :], conv[rows, cw : cw + st])
        for h in range(cw // hd):
            gap = jnp.where(lower, cum_cs[b][:, h : h + 1] - cum_rs[b][h : h + 1, :], -jnp.inf)
            wm = g * jnp.exp(gap) * st_rs[b][h : h + 1, :]
            top, low = halves(wm)
            v = conv[rows, h * hd : (h + 1) * hd]
            scan[rows, h * hd : (h + 1) * hd] = jnp.dot(top, v, preferred_element_type=F32) + jnp.dot(
                low, v, preferred_element_type=F32
            )

    window = lax.shift_left(jnp.int32(2), tp)
    back = (
        lax.broadcasted_iota(jnp.int32, (blk, blk + raw0), 0)
        + raw0
        - lax.broadcasted_iota(jnp.int32, (blk, blk + raw0), 1)
    )
    band = jnp.where((back >= 0) & (back < window), 1.0, 0.0).astype(BF)

    def pool(b):
        rows = slice(b * blk, (b + 1) * blk)
        sums = jnp.dot(band, extp[b * blk : (b + 1) * blk + raw0, :].astype(BF), preferred_element_type=F32)
        pos = (me * n + b * blk + lax.broadcasted_iota(jnp.int32, (blk, cw), 0)).astype(F32)
        counts = jnp.minimum(pos + 1.0, window.astype(F32))
        pooled = (sums / counts - extp[b * blk + raw0 : (b + 1) * blk + raw0, :]).astype(BF)
        pbuf[pslot, rows, :] = (
            jnp.dot(pooled, mixb[0], preferred_element_type=F32) * par[0, 16:17, 0:cw]
        ).astype(BF)

    rows_of = (sbuf, pbuf)

    def rcopy(k, r, way, src=None):
        to = ({"c_": 1 - c}, {"x_": 1 - x}, {"y_": 1 - y})[way]
        src = rows_of[k].at[r] if src is None else src
        return copy(src, rows_of[k].at[r], p_ss.at[(k * T + r) * 3 + way], p_rs.at[k * T + r], **to)

    def qcopy(i):
        to = ({"c_": 1 - c}, {"x_": 1 - x}, {"x_": 1 - x, "c_": 1 - c}, {})[i]
        return copy(sq_buf.at[pslot], sq_buf.at[tp], q_ss.at[i], q_rs.at[tp], **{"y_": c, **to})

    def rows_out(k, do):
        @pl.when(moved)
        def _():
            do(rcopy(k, tp, 2, rows_of[k].at[T]))

        @pl.when(kept)
        def _():
            do(rcopy(k, tp, 1))
            do(rcopy(k, tp, 0))

    def rows_on(k, do, wait=True):
        @pl.when(kept)
        def _():
            other = 2 * x + 1 - y
            if wait:
                rcopy(k, other, 0).wait_recv()
            do(rcopy(k, other, 1))
            do(rcopy(k, other, 0))

    def rows_over(k, do, wait=True):
        @pl.when(kept)
        def _():
            for r in (2 * (1 - x) + y, 2 * (1 - x) + 1 - y):
                if wait:
                    rcopy(k, r, 0).wait_recv()
                do(rcopy(k, r, 0))

    def squares(do):
        for i in range(3):
            do(qcopy(i))

        @pl.when(moved)
        def _():
            do(qcopy(3))

    def gates():
        for r0, rows in tiles():
            d = jnp.dot(nbuf[0, rows, :], gbuf[0], preferred_element_type=F32)
            for i in range(1, S):
                d = d + jnp.dot(nbuf[i, rows, :], gbuf[i], preferred_element_type=F32)
            low = d.astype(BF)
            keep(extp, r0, low[:, 0:cw])
            gateb[r0 : r0 + mt, :] = low[0:mt, cw:]

    def pools():
        for b in range(blocks):
            pool(b)
        rows_out(1, start)

    def xpair():
        return copy(xs.at[0], xr.at[Z - 1], x_ss.at[0], x_rs.at[Z - 1], c_=1 - c)

    def xline(k):
        return copy(xs.at[1], xr.at[z], x_ss.at[k], x_rs.at[z], z_=z + k)

    def xlines(do):
        for k in range(1, Z):
            @pl.when(z + k < Z)
            def _():
                do(xline(k))

    def put(i):
        xs[i, 0:st, :] = run
        xs[i, st:, :] = jnp.broadcast_to(dec, (xs.shape[1] - st, cw))

    put(0)
    xpair().start()

    @pl.when(kept)
    def _():
        pump(1, 3, start)

    @pl.when(moved)
    def _():
        pump(1, 2, start, when=jnp.logical_not(middle))

    for b in range(blocks // 2):
        inner(b)
    xpair().wait_recv()
    other, odec = xr[Z - 1, 0:st, :], xr[Z - 1, st : st + 1, :]
    later = c == 1
    own_s, own_d = jnp.where(later, other, 0.0), jnp.where(later, odec, 1.0)
    run = jnp.where(later, other * dec + run, run * odec + other)
    dec = dec * odec
    put(1)
    xlines(start)
    ofrom(1, middle)

    for b in range(blocks // 2, blocks):
        inner(b)
    opass(0, kept)

    @pl.when(moved)
    def _():
        pump(1, 3, start)

    ofrom(1, jnp.logical_not(middle))
    partners(1)
    gates()

    @pl.when(moved)
    def _():
        swap(3).wait_recv()

    pools()
    opass(0, moved)
    in_s = jnp.zeros((st, cw), F32)
    for p in range(Z - 1):
        @pl.when(z > p)
        def _():
            copy(xs.at[1], xr.at[p], x_ss.at[1], x_rs.at[p], c_=1 - c).wait_recv()

        in_s = jnp.where(z > p, in_s * xr[p, st : st + 1, :] + xr[p, 0:st, :], in_s)
    in_s = in_s * own_d + own_s

    for b in range(blocks):
        rows = slice(b * blk, (b + 1) * blk)
        top, low = halves(pres[b] + offs[b] * in_s)
        rd = conv[rows, cw + st :]
        carried = jnp.dot(rd, top, preferred_element_type=F32) + jnp.dot(rd, low, preferred_element_type=F32)
        out_b = scan[rows, :] + carried * expd[rows, :] + skips * conv[rows, 0:cw].astype(F32)
        gt = gateb[rows, :].astype(F32)
        gated = out_b * (gt * jax.nn.sigmoid(gt))
        sq_buf[pslot, :, rows] = bt(jnp.ones((8, cw), F32), gated * gated, precision=HIGH)
        sbuf[pslot, rows, :] = (gated * par[0, 16:17, cw : 2 * cw]).astype(BF)

    rows_out(0, start)
    squares(start)
    opass(1)
    olate()
    oend(0)
    rows_on(1, start)
    ofar(0, start)
    oend(1)
    rows_on(0, start)
    if TWIN:
        otwin(0, start)
    ofar(1, start)
    rows_over(1, start)
    rows_over(0, start)
    if TWIN > 1:
        otwin(1, start)
    @pl.when(moved)
    def _():
        for k in range(2):
            for r in range(T):
                rcopy(k, r, 0).wait_recv()

    for r in range(T):
        @pl.when((tp != r) | moved)
        def _():
            copy(sq_buf.at[r], sq_buf.at[r], q_ss.at[0], q_rs.at[r], c_=1 - c).wait_recv()

    for q in range(T):
        i = (1 - y) * T + q
        known = (q == 2 * x + 1 - y) & (TWIN > 0) | (q == 2 * x + y) & (TWIN > 1)

        @pl.when(jnp.logical_not(relays(0) & known))
        def _():
            copy(obuf.at[i], obuf.at[i], o_ss.at[0], o_rs.at[i], y_=1 - y).wait_recv()

    sq = sum(sq_buf[r] for r in range(T))
    rs_row = lax.rsqrt(sq / (cw * T) + EPSILON)
    rs_cols = [bt(eye, rs_row[:, b * blk : (b + 1) * blk], precision=HIGH)[:, 0:1] for b in range(blocks)]
    for r0 in range(0, n, mt):
        rows = slice(r0, r0 + mt)
        rs = jnp.concatenate(rs_cols[r0 // blk : (r0 + mt) // blk], axis=0)
        for j in range(2):
            p = jnp.dot(pbuf[0, rows, :], obuf[j * T, 0:cw, :], preferred_element_type=F32)
            s = jnp.dot(sbuf[0, rows, :], obuf[j * T, cw:, :], preferred_element_type=F32)
            for q in range(1, T):
                p = p + jnp.dot(pbuf[q, rows, :], obuf[j * T + q, 0:cw, :], preferred_element_type=F32)
                s = s + jnp.dot(sbuf[q, rows, :], obuf[j * T + q, cw:, :], preferred_element_type=F32)
            out[rows, j * oc : (j + 1) * oc] = (p + rs * s).astype(out.dtype)

    for k in range(2):
        source(k, done)
        for d in range(1, Z):
            pump(k, d, done, wait=False)
        rows_out(k, done)
        rows_on(k, done, wait=False)
        rows_over(k, done, wait=False)
    oall(done)
    squares(done)
    acopy(1).wait_send()
    acopy(2).wait_send()

    @pl.when(moved)
    def _():
        acopy(0).wait_send()
        for i in range(4):
            swap(i).wait_send()
        aforward(0).wait_send()

    @pl.when(kept)
    def _():
        aforward(1).wait_send()

    @pl.when(jnp.logical_not(hub))
    def _():
        ohub().wait_send()

    xpair().wait_send()
    xlines(done)

    hsends(done)


def fits(S, T, shapes):
    n, da = shapes[0]
    kd, cw = shapes[2]
    st = shapes[5][1]
    oc = shapes[18][1]
    heads = shapes[7][1]
    taps = shapes[10][0]
    return (
        T == 4 == POOL_GROUPS and S == 2 * T and st == SSM_STATE and taps <= 8 and heads <= 8
        and cw == heads * SSM_STATE and n % 256 == 0 and n % SCAN_BLOCK == 0 and n >= 2 * cw
        and oc % 128 == 0 and kd % 128 == 0 and da % kd == 0 and da * T == kd * S and kd <= cw + 2 * st
        and cw % 128 == 0 and oc * 2 == da
    )


def fused(
    S, T, activations, norm_gain, pool_weight, gate_weight, value_weight, key_weight, read_weight,
    step_weight, pool_mix, pool_scale, taps_value, taps_key, taps_read, step_bias, decay_log,
    decay_extra, skip_scale, state_gain, out_pool_weight, out_state_weight,
):
    n, da = activations.shape
    kd, cw = pool_weight.shape
    st = key_weight.shape[1]
    oc = out_pool_weight.shape[1]
    hp = 16
    args = (
        activations, norm_gain.reshape(-1, 128), pool_weight, gate_weight, value_weight, key_weight.T, read_weight.T,
        step_weight.T, pool_mix, pool_scale[None, :], taps_value, taps_key, taps_read, step_bias[None, :], decay_log[None, :],
        decay_extra.T, skip_scale[None, :], state_gain[None, :],
        out_pool_weight, out_state_weight,
    )
    vc = cw + 2 * st
    V = pltpu.VMEM
    D = pltpu.SemaphoreType.DMA
    scratch = [
        V((S + 1, kd + hp, vc), BF), V((S + 1, kd, 2 * cw), BF), V((2 * T + 3, 2 * cw, oc), BF),
        V((T + 1, n + 16, da), BF), V((2, cw, cw), BF), V((2, 32, n), F32),
        V((S, n + 16, kd), BF), V((n + 16, vc), F32), V((n + 16, cw), F32), V((n, cw), BF), V((n, vc), BF),
        V((T, 16, da), BF), V((n, cw), F32),
        V((2, st + 8, cw), F32), V((S // 2, st + 8, cw), F32),
        V((T + 1, 8, n), F32), V((T + 1, n, cw), BF), V((T + 1, n, cw), BF), V((n, cw), F32),
        D((10 * S,)), D((2 * S,)), D((29,)), D((2 * T + 3,)), D((5,)), D((T,)), D((4,)), D((2,)),
        D((4,)), D((T,)), D((S // 2,)), D((S // 2,)), D((4,)), D((T,)), D((6 * T,)), D((2 * T,)),
    ]
    return pl.pallas_call(
        functools.partial(mixer_kernel, S, T),
        out_shape=jax.ShapeDtypeStruct((n, da), BF),
        in_specs=[pl.BlockSpec(memory_space=pltpu.VMEM)] * len(args),
        out_specs=pl.BlockSpec(memory_space=pltpu.VMEM),
        scratch_shapes=scratch,
        compiler_params=pltpu.CompilerParams(
            collective_id=0, has_side_effects=True, vmem_limit_bytes=60 * 1024 * 1024
        ),
    )(*args)


def solution(mesh):
    placed = (
        P("sp", "tp"),
        P("tp"),
        P("sp", "tp"),
        P("sp", "tp"),
        P("sp", "tp"),
        P("sp", "tp"),
        P("sp", "tp"),
        P("sp", "tp"),
        P("tp", None, None),
        P("tp"),
        P(None, "tp"),
        P(None, "tp"),
        P(None, "tp"),
        P("tp"),
        P("tp"),
        P("sp", "tp"),
        P("tp"),
        P("tp"),
        P("tp", "sp"),
        P("tp", "sp"),
    )
    S, T = mesh.shape["sp"], mesh.shape["tp"]

    def chosen(*args):
        if fits(S, T, [a.shape for a in args]):
            return fused(S, T, *args)
        return local(*args)

    return jax.shard_map(
        chosen, mesh=mesh, in_specs=placed, out_specs=P("sp", "tp"), check_vma=False
    )
```

```python
import functools

import jax
import jax.numpy as jnp
from jax import lax
from jax.experimental import pallas as pl
from jax.experimental.pallas import tpu as pltpu
from jax.sharding import PartitionSpec as P

SSM_STATE = 64
POOL_GROUPS = 4
SCAN_BLOCK = 128
MIX_W = 1024


EPSILON = 1e-06
HIGH = lax.Precision.HIGHEST


def shifted(value, axis, steps):
    count = lax.axis_size(axis)
    leading, last = (max(0, -steps), min(count, count - steps))
    return lax.ppermute(value, axis, [(source, source + steps) for source in range(leading, last)])


def carried_in(part, axis, combine, identity):
    place = lax.axis_index(axis)
    gathered = jax.tree.map(lambda a: lax.all_gather(a, axis), part)
    state = jax.tree.map(lambda a, e: jnp.zeros_like(a) + jnp.asarray(e, a.dtype), part, identity)

    def one(step, state):
        return combine(
            state, jax.tree.map(lambda a: lax.dynamic_index_in_dim(a, step, 0, False), gathered)
        )

    return lax.fori_loop(0, place, one, state)


def backward_kernel(extended, taps):
    width = taps.shape[0]
    length = extended.shape[0] - (width - 1)
    widened_rows = extended.astype(jnp.float32)
    total = jnp.zeros((length, extended.shape[1]), jnp.float32)
    for offset in range(width):
        total = total + taps[offset][None, :] * widened_rows[offset : offset + length]
    return jax.nn.silu(total).astype(jnp.bfloat16)


def combine_states(preceding_token, later):
    return (preceding_token[0] * later[0], preceding_token[1] * later[0][:, None, None] + later[1])


def local(
    activations,
    norm_gain,
    pool_weight,
    gate_weight,
    value_weight,
    key_weight,
    read_weight,
    step_weight,
    pool_mix,
    pool_scale,
    taps_value,
    taps_key,
    taps_read,
    step_bias,
    decay_log,
    decay_extra,
    skip_scale,
    state_gain,
    out_pool_weight,
    out_state_weight,
):
    length = activations.shape[0]
    cluster_span = pool_weight.shape[1]
    local_mix = gate_weight.shape[1]
    local_state = key_weight.shape[1]
    local_heads = step_weight.shape[1]
    joined = jnp.concatenate(
        [pool_weight, gate_weight, value_weight, key_weight, read_weight, step_weight], axis=1
    )
    in_weight = lax.all_gather(joined, "sp", axis=0, tiled=True)
    whole, gains = (
        lax.all_gather(activations, "tp", axis=1, tiled=True),
        lax.all_gather(norm_gain, "tp", axis=0, tiled=True),
    )
    widened_rows = whole.astype(jnp.float32)
    normed = (
        widened_rows
        * lax.rsqrt(jnp.mean(widened_rows * widened_rows, axis=-1, keepdims=True) + EPSILON)
        * gains.astype(jnp.float32)
    ).astype(jnp.bfloat16)
    projected = jnp.dot(normed, in_weight, preferred_element_type=jnp.float32)
    column = 0
    pool_in = projected[:, column : column + cluster_span].astype(jnp.bfloat16)
    column = column + cluster_span
    gate_in = projected[:, column : column + local_mix].astype(jnp.bfloat16)
    column = column + local_mix
    raw_value = projected[:, column : column + local_mix].astype(jnp.bfloat16)
    column = column + local_mix
    raw_key = projected[:, column : column + local_state].astype(jnp.bfloat16)
    column = column + local_state
    raw_read = projected[:, column : column + local_state].astype(jnp.bfloat16)
    column = column + local_state
    step_raw = projected[:, column : column + local_heads]
    raw_joined = jnp.concatenate([raw_value, raw_key, raw_read], axis=1)
    reach = 2**POOL_GROUPS - 1
    width = taps_value.shape[0]
    prior_pool, prior_joined = shifted(
        (pool_in[length - reach :], raw_joined[length - width + 1 :]), "sp", 1
    )
    group = lax.axis_index("tp")
    running = jnp.concatenate([prior_pool, pool_in], axis=0).astype(jnp.float32)
    levels = []
    for level in range(POOL_GROUPS):
        stride = 2**level
        running = running[stride:] + running[:-stride]
        levels.append(running[running.shape[0] - length :])
    window_sum = lax.dynamic_index_in_dim(jnp.stack(levels), group, 0, keepdims=False)
    window = jnp.exp2((group + 1).astype(jnp.float32))
    position = (lax.axis_index("sp") * length + jnp.arange(length, dtype=jnp.int32)).astype(
        jnp.float32
    )
    counts = jnp.minimum(position + 1.0, window)
    pooled = (window_sum / counts[:, None] - pool_in.astype(jnp.float32)).astype(jnp.bfloat16)
    pool_out = (
        jnp.dot(pooled, pool_mix[0], preferred_element_type=jnp.float32) * pool_scale
    ).astype(jnp.bfloat16)
    all_taps = jnp.concatenate([taps_value, taps_key, taps_read], axis=1)
    convolved = backward_kernel(jnp.concatenate([prior_joined, raw_joined], axis=0), all_taps)
    head_value = convolved[:, :local_mix]
    key_vectors = convolved[:, local_mix : local_mix + local_state]
    read_vectors = convolved[:, local_mix + local_state :]
    head_dim = local_mix // local_heads
    groups_here = local_state // SSM_STATE
    repeat = local_heads // groups_here
    blocks = length // SCAN_BLOCK
    step_size = jax.nn.softplus(step_raw + step_bias)
    log_decay = -jnp.exp(decay_log) * step_size + decay_extra
    value_heads = head_value.astype(jnp.float32).reshape(length, local_heads, head_dim)
    value_blocks = value_heads.reshape(blocks, SCAN_BLOCK, local_heads, head_dim)
    key_blocks = jnp.repeat(
        key_vectors.astype(jnp.float32).reshape(length, groups_here, SSM_STATE), repeat, axis=1
    ).reshape(blocks, SCAN_BLOCK, local_heads, SSM_STATE)
    read_blocks = jnp.repeat(
        read_vectors.astype(jnp.float32).reshape(length, groups_here, SSM_STATE), repeat, axis=1
    ).reshape(blocks, SCAN_BLOCK, local_heads, SSM_STATE)
    step_blocks = step_size.reshape(blocks, SCAN_BLOCK, local_heads)
    running_decay = jnp.cumsum(log_decay.reshape(blocks, SCAN_BLOCK, local_heads), axis=1)
    lower = jnp.arange(SCAN_BLOCK)[:, None] >= jnp.arange(SCAN_BLOCK)[None, :]
    gaps = jnp.where(
        lower[None, :, :, None],
        running_decay[:, :, None, :] - running_decay[:, None, :, :],
        -jnp.inf,
    )
    weights = jnp.einsum("blhn,bshn->blsh", read_blocks, key_blocks, precision=HIGH) * jnp.exp(gaps)
    scaled_value = value_blocks * step_blocks[..., None]
    inner = jnp.einsum("blsh,bshp->blhp", weights, scaled_value, precision=HIGH)
    block_ends = running_decay[:, -1, :]
    trailing = jnp.exp(block_ends[:, None, :] - running_decay)
    fresh = jnp.einsum("bshn,bsh,bshp->bhpn", key_blocks, trailing, scaled_value, precision=HIGH)

    def advance(carry, inputs):
        block_decay, block_state = inputs
        return (carry * block_decay[:, None, None] + block_state, carry)

    local_total, prefix = lax.scan(
        advance,
        jnp.zeros((local_heads, head_dim, SSM_STATE), jnp.float32),
        (jnp.exp(block_ends), fresh),
    )
    offsets = jnp.cumsum(block_ends, axis=0) - block_ends
    device_decay = jnp.exp(offsets[-1] + block_ends[-1])
    incoming_decay, incoming = carried_in(
        (device_decay, local_total),
        "sp",
        combine_states,
        (jnp.ones_like(device_decay), jnp.zeros_like(local_total)),
    )
    from_device = running_decay + offsets[:, None, :]
    local_off = (
        jnp.einsum("blhn,bhpn->blhp", read_blocks, prefix, precision=HIGH)
        * jnp.exp(running_decay)[..., None]
    )
    far_off = (
        jnp.einsum("blhn,hpn->blhp", read_blocks, incoming, precision=HIGH)
        * jnp.exp(from_device)[..., None]
    )
    scan_out = (inner + local_off + far_off).reshape(length, local_heads, head_dim) + skip_scale[
        None, :, None
    ] * value_heads
    gated = scan_out.reshape(length, local_mix) * jax.nn.silu(gate_in.astype(jnp.float32))
    gate_squares = lax.psum(jnp.sum(gated * gated, axis=-1), "tp")
    state_out = (gated * lax.rsqrt(gate_squares / MIX_W + EPSILON)[:, None] * state_gain).astype(
        jnp.bfloat16
    )
    branch_rows = jnp.concatenate([pool_out, state_out], axis=1)
    out_weight = jnp.concatenate([out_pool_weight, out_state_weight], axis=0)
    terms = jnp.dot(
        branch_rows,
        lax.all_gather(out_weight, "sp", axis=1, tiled=True),
        preferred_element_type=jnp.float32,
    )
    result = lax.psum_scatter(terms, "tp", scatter_dimension=1, tiled=True)
    return result.astype(jnp.bfloat16)


BF = jnp.bfloat16
F32 = jnp.float32
MESH = pl.DeviceIdType.MESH


def flip(index, mask):
    bit = 1
    while bit <= mask:
        if mask & bit:
            index = index + bit - 2 * bit * lax.rem(lax.div(index, bit), 2)
        bit *= 2
    return index


def bt(a, b, **kw):
    return lax.dot_general(a, b, (((1,), (1,)), ((), ())), preferred_element_type=F32, **kw)


def halves(x):
    top = x.astype(BF)
    return top, (x - top.astype(F32)).astype(BF)


TWIN = 2


def mixer_kernel(
    S, T,
    act, gain, pool_w, gate_w, value_w, key_w, read_w, step_t, mix, scale, taps_v, taps_k, taps_r,
    bias, dlog, extra_t, skip, sgain, opool, ostate,
    out,
    vbuf, gbuf, obuf, abuf, mixb, par, nbuf, extv, extp, gateb, conv, hbuf, scan, xs, xr,
    sq_buf, pbuf, sbuf, expd,
    b_ss, b_rs, o_ss, o_rs, a_ss, a_rs, t_ss, t_rs, h_ss, h_rs, x_ss, x_rs, q_ss, q_rs, p_ss, p_rs,
):
    n, da = act.shape
    kd, cw = pool_w.shape
    st = key_w.shape[0]
    heads = step_t.shape[0]
    hp = vbuf.shape[1] - kd
    vc = cw + 2 * st
    oc = opool.shape[1]
    blk = SCAN_BLOCK
    blocks = n // blk
    hd = SSM_STATE
    Z = S // 2
    sp, tq = lax.axis_index("sp"), lax.axis_index("tp")
    z, y = lax.div(sp, 2), lax.rem(sp, 2)
    x, c = lax.div(tq, 2), lax.rem(tq, 2)
    me, tp = 2 * z + c, 2 * x + y
    off = lax.rem(y + c, 2)
    moved, kept = off == 1, off == 0
    slot = me + off * (S - me)
    aslot = tq + off * (T - tq)
    pslot = tp + off * (T - tp)
    hubs = (tq == z, 2 * (1 - x) + c == z)
    hub = hubs[0] | hubs[1]
    turn = lax.rem(y + c, 2)
    oslot = jnp.where(hubs[0], y * T + tq, jnp.where(hubs[1], 2 * T + 1 + turn, 2 * T))

    def dev(z_=z, y_=y, x_=x, c_=c):
        return {"sp": 2 * z_ + y_, "tp": 2 * x_ + c_}

    def copy(src, dst, ss, rs, **to):
        return pltpu.make_async_remote_copy(
            src_ref=src, dst_ref=dst, send_sem=ss, recv_sem=rs, device_id=dev(**to), device_id_type=MESH
        )

    barrier = pltpu.get_barrier_semaphore()

    def greet(**to):
        pl.semaphore_signal(barrier, inc=1, device_id=dev(**to), device_id_type=MESH)

    for dz in range(Z):
        for k in range(8):
            if dz or k:
                greet(
                    z_=lax.rem(z + dz, Z), y_=1 - y if k & 4 else y, x_=1 - x if k & 2 else x,
                    c_=1 - c if k & 1 else c,
                )

    eye_kd = jnp.where(
        lax.broadcasted_iota(jnp.int32, (kd, kd), 0) == lax.broadcasted_iota(jnp.int32, (kd, kd), 1), 1.0, 0.0
    ).astype(BF)
    pick = jnp.where(
        lax.broadcasted_iota(jnp.int32, (hp, heads), 0) == lax.broadcasted_iota(jnp.int32, (hp, heads), 1), 1.0, 0.0
    ).astype(F32)
    vbuf[slot, 0:kd, 0:cw] = value_w[...]
    vbuf[slot, 0:kd, cw:] = bt(eye_kd, jnp.concatenate([key_w[...], read_w[...]], axis=0)).astype(BF)
    vbuf[slot, kd:, :] = jnp.zeros((hp, vc), BF)
    vbuf[slot, kd:, 0:kd] = jnp.dot(pick.astype(BF), step_t[...], preferred_element_type=F32).astype(BF)
    abuf[aslot, 0:n, :] = act[...]
    for i in range(gain.shape[0]):
        g = jnp.broadcast_to(gain[i : i + 1, :].astype(F32), (16, gain.shape[1]))
        abuf[aslot, n : n + 16, i * gain.shape[1] : (i + 1) * gain.shape[1]] = g.astype(BF)

    gbuf[slot, :, 0:cw] = pool_w[...]
    gbuf[slot, :, cw:] = gate_w[...]
    obuf[oslot, 0:cw, :] = opool[...]
    obuf[oslot, cw:, :] = ostate[...]
    mixb[off] = mix[0]
    par[off] = jnp.zeros(par.shape[1:], F32)
    par[off, 0:heads, :] = extra_t[...]
    par[off, 16:17, 0:cw] = scale[...]
    par[off, 16:17, cw : 2 * cw] = sgain[...]
    par[off, 17:18, 0:heads] = bias[...]
    par[off, 18:19, 0:heads] = dlog[...]
    par[off, 19:20, 0:heads] = skip[...]
    width = taps_v.shape[0]
    par[off, 24 : 24 + width, 0:cw] = taps_v[...]
    par[off, 24 : 24 + width, cw : cw + st] = taps_k[...]
    par[off, 24 : 24 + width, cw + st : vc] = taps_r[...]
    pl.semaphore_wait(barrier, S * T - 1)

    raw0 = hbuf.shape[1]
    own_halo = (y == 0) & (c == 1)

    @pl.when(own_halo)
    def _():
        hbuf[tq] = act[n - raw0 :, :]

    @pl.when(me == 0)
    def _():
        hbuf[...] = jnp.zeros(hbuf.shape, BF)

    middle = (z == 1) | (z == Z - 2)
    streams = (vbuf, gbuf)

    def bcopy(k, i, way):
        to = ({"c_": 1 - c}, {"z_": z + 1}, {"z_": z - 1}, {"z_": z + 2}, {"z_": z - 2})[way]
        ref = streams[k].at[i]
        return copy(ref, ref, b_ss.at[(k * S + i) * 5 + way], b_rs.at[k * S + i], **to)

    def arrived(k, i):
        bcopy(k, i, 0).wait_recv()

    def source(k, do):
        ways = [(1, z < Z - 1), (2, z > 0)]
        if k:
            ways = [(3, moved & (z == 0)), (4, moved & (z == Z - 1))] + ways
        for way, when in ways:
            @pl.when(when)
            def _():
                do(bcopy(k, me, way))

        do(bcopy(k, me, 0))

    def start(d):
        d.start()

    def done(d):
        d.wait_send()

    def pump(k, d, do, wait=True, when=True):
        right, left = z < Z - 1, z > 0
        if k and d == 1:
            right, left = right & (kept | (z > 1)), left & (kept | (z < Z - 2))

        @pl.when((z >= d) & when)
        def _():
            i = 2 * (z - d) + c
            if wait:
                arrived(k, i)

            @pl.when(right)
            def _():
                do(bcopy(k, i, 1))

            do(bcopy(k, i, 0))

        @pl.when((z + d < Z) & when)
        def _():
            i = 2 * (z + d) + c
            if wait:
                arrived(k, i)

            @pl.when(left)
            def _():
                do(bcopy(k, i, 2))

            do(bcopy(k, i, 0))

    def partners(k):
        for p in range(Z):
            arrived(k, 2 * p + 1 - c)

    def swap(i):
        src, dst, rs = (
            (vbuf.at[S], vbuf.at[sp], b_rs.at[sp]),
            (par.at[1], par.at[0], t_rs.at[0]),
            (gbuf.at[S], gbuf.at[sp], b_rs.at[S + sp]),
            (mixb.at[1], mixb.at[0], t_rs.at[1]),
        )[i]
        return copy(src, dst, t_ss.at[i], rs, y_=c, c_=y)

    def acopy(way):
        to = ({"c_": y}, {"x_": 1 - x, "c_": y}, {"y_": 1 - y, "c_": y})[way]
        return copy(abuf.at[aslot], abuf.at[tq], a_ss.at[way], a_rs.at[tq], **to)

    head = n // 2 + 16

    def aforward(i):
        t, rows, rs, to = (
            (2 * x + 1 - c, pl.ds(0, n + 16), None, {"x_": 1 - x}),
            (2 * (1 - x) + c, pl.ds(0, head), None, {"y_": 1 - y}),
            (2 * x + c, pl.ds(head, n + 16 - head), T, {"x_": 1 - x}),
        )[i]
        ref = abuf.at[t, rows]
        return copy(ref, ref, a_ss.at[3 + i], a_rs.at[t if rs is None else rs], **to)

    def afar():
        t = 2 * (1 - x) + c
        for rows, rs in ((pl.ds(0, head), t), (pl.ds(head, n + 16 - head), T)):
            ref = abuf.at[t, rows]
            copy(ref, ref, a_ss.at[0], a_rs.at[rs], x_=1 - x).wait_recv()

    def agot(t):
        copy(abuf.at[t], abuf.at[t], a_ss.at[0], a_rs.at[t], x_=1 - x).wait_recv()

    def hcopy(k):
        return copy(
            abuf.at[aslot, pl.ds(n - raw0, raw0)], hbuf.at[tq], h_ss.at[k], h_rs.at[tq],
            z_=z + y, y_=k // 2, x_=k % 2, c_=1 - y,
        )

    def hsends(do):
        @pl.when(sp < S - 1)
        def _():
            for k in range(4):
                @pl.when(jnp.logical_not(own_halo & (y == k // 2) & (x == k % 2)))
                def _():
                    do(hcopy(k))

    def hgot():
        @pl.when(me > 0)
        def _():
            for t in range(T):
                @pl.when(jnp.logical_not(own_halo & (tq == t)))
                def _():
                    copy(hbuf.at[t], hbuf.at[t], h_ss.at[0], h_rs.at[t], x_=1 - x).wait_recv()

    def oquarter(j):
        return 2 * x + (y if j == 0 else 1 - y)

    def oslots(line, j):
        return 2 * T + 1 + j if line else y * T + oquarter(j)

    def ohub():
        home = lax.div(z, 2) == x
        dst = jnp.where(home, y * T + tq, 2 * T + 1 + turn)
        return copy(obuf.at[2 * T], obuf.at[dst], o_ss.at[0], o_rs.at[dst], c_=1 - c)

    def ocopy(line, j, way, final=False):
        to = (
            {"z_": z + 1}, {"z_": z - 1}, {"z_": z + 2}, {"z_": z - 2},
            {"x_": 1 - x} if line else {"y_": 1 - y},
        )[way]
        if final and line:
            to = {"x_": 1 - x, **to}
        i = oslots(line, j)
        dst = i if way < 4 and not final else y * T + oquarter(j)
        return copy(obuf.at[i], obuf.at[dst], o_ss.at[1 + (2 * line + j) * 6 + way], o_rs.at[dst], **to)

    def owait(line, j):
        i = oslots(line, j)
        copy(obuf.at[i], obuf.at[i], o_ss.at[0], o_rs.at[i], x_=1 - x).wait_recv()

    def across(line, j, do):
        if not line:
            do(ocopy(line, j, 4))

    def over(line, j, do):
        if line:
            do(ocopy(line, j, 4))

    def osend(line, j, do):
        for way, final, when in (
            (2, False, z == 0), (3, False, z == Z - 1), (0, False, z == 1), (1, True, z == 1),
            (1, False, z == Z - 2), (0, True, z == Z - 2),
        ):
            @pl.when(when)
            def _():
                do(ocopy(line, j, way, final))

    def center(line):
        return 2 * (1 - x) + c if line else tq

    def relays(line):
        h = center(line)
        return ((z == Z - 2) & (h < 2)) | ((z == 1) & (h > 1))

    def orelay(line, j, do):
        h = center(line)
        for way, when in ((0, h < 2), (1, h > 1), (1, h == 0), (0, h == T - 1)):
            @pl.when(when)
            def _():
                do(ocopy(line, j, way, True))

    def ofrom(j, when=True):
        for line in range(2):
            @pl.when(hubs[line] & when)
            def _():
                osend(line, j, start)

    def ocross():
        for line in range(2):
            @pl.when(hubs[line])
            def _():
                for j in range(2):
                    @pl.when(turn != j)
                    def _():
                        owait(line, j)

                    over(line, j, start)
                    across(line, j, start)

    def opass(j, when=True):
        for line in range(2):
            @pl.when(relays(line) & when)
            def _():
                owait(line, j)
                orelay(line, j, start)
                over(line, j, start)

                @pl.when(kept)
                def _():
                    across(line, j, start)

    def olate(j):
        @pl.when(relays(0) & moved)
        def _():
            across(0, j, start)

    def oend(j):
        @pl.when(jnp.logical_not(hubs[0] | relays(0)))
        def _():
            owait(0, j)

            @pl.when(jnp.logical_not(last & (j < TWIN)))
            def _():
                across(0, j, start)

    last = ((z == Z - 1) & (x == 0)) | ((z == 0) & (x == 1))

    def otwin(j, do, wait=True):
        @pl.when(relays(0))
        def _():
            i = (1 - y) * T + 2 * x + (1 - y if j == 0 else y)
            d = copy(obuf.at[i], obuf.at[i], o_ss.at[27 + j], o_rs.at[i], z_=z + 1 - 2 * x)
            if wait:
                d.wait_recv()
            do(d)

    def ofar(j, do, wait=True):
        i = y * T + 2 * (1 - x) + (y if j == 0 else 1 - y)
        d = copy(obuf.at[i], obuf.at[i], o_ss.at[25 + j], o_rs.at[i], y_=1 - y)
        if wait:
            d.wait_recv()
        do(d)

    def oall(do):
        for j in range(2):
            ofar(j, do, False)

        for line in range(2):
            for j in range(2):
                @pl.when(hubs[line])
                def _():
                    osend(line, j, do)

                @pl.when(relays(line))
                def _():
                    orelay(line, j, do)

                @pl.when(hubs[line] | relays(line))
                def _():
                    over(line, j, do)

                @pl.when(jnp.logical_not(last & (j < TWIN)))
                def _():
                    across(line, j, do)

        for j in range(TWIN):
            otwin(j, do, False)

    @pl.when(moved)
    def _():
        swap(0).start()

    acopy(1).start()
    hsends(start)

    @pl.when(moved)
    def _():
        acopy(2).start()
        acopy(0).start()
        swap(2).start()
        swap(1).start()

        @pl.when(jnp.logical_not(hub))
        def _():
            ohub().start()

    @pl.when(moved)
    def _():
        arrived(0, me)

    source(0, start)

    @pl.when(kept)
    def _():
        source(1, start)

    pump(0, 1, start)

    @pl.when(kept)
    def _():
        acopy(2).start()
        agot(2 * (1 - x) + c)
        aforward(1).start()

        @pl.when(jnp.logical_not(hub))
        def _():
            ohub().start()

    @pl.when(moved)
    def _():
        agot(2 * x + 1 - c)
        aforward(0).start()

    pump(0, 2, start)

    @pl.when(moved)
    def _():
        agot(2 * x + c)
        aforward(2).start()

    pump(0, 3, start)

    @pl.when(moved)
    def _():
        swap(3).start()
        arrived(1, me)
        source(1, start)

    @pl.when(kept)
    def _():
        pump(1, 1, start)

    partners(0)
    @pl.when(moved)
    def _():
        swap(1).wait_recv()

    def column(row):
        return bt(pick, jnp.broadcast_to(row, (8, heads)), precision=HIGH)[:, 0:1]

    bias_c = column(par[0, 17:18, 0:heads])
    rate_c = -jnp.exp(column(par[0, 18:19, 0:heads]))
    r_i = lax.broadcasted_iota(jnp.int32, (blk, blk), 0)
    c_i = lax.broadcasted_iota(jnp.int32, (blk, blk), 1)
    eye = jnp.where(r_i == c_i, 1.0, 0.0).astype(F32)
    lower = r_i >= c_i
    expand = jnp.where(
        lax.broadcasted_iota(jnp.int32, (hp, cw), 1) // hd == lax.broadcasted_iota(jnp.int32, (hp, cw), 0), 1.0, 0.0
    ).astype(F32)
    skips = jnp.dot(
        jnp.broadcast_to(par[0, 19:20, 0:heads], (8, heads)), expand[0:heads, :],
        precision=HIGH, preferred_element_type=F32,
    )[0:1, :]
    eye_st = jnp.where(
        lax.broadcasted_iota(jnp.int32, (st, st), 0) == lax.broadcasted_iota(jnp.int32, (st, st), 1), 1.0, 0.0
    ).astype(BF)

    def thirds(v):
        top = v.astype(BF)
        rest = v - top.astype(F32)
        mid = rest.astype(BF)
        return jnp.concatenate([top, mid, (rest - mid.astype(F32)).astype(BF)], axis=1)

    upper = jnp.concatenate([jnp.where(r_i <= c_i, 1.0, 0.0).astype(BF)] * 3, axis=0)
    row = lax.rem(lax.broadcasted_iota(jnp.int32, (3 * blocks * hp, blocks * cw), 0), blocks * hp)
    col = lax.broadcasted_iota(jnp.int32, (3 * blocks * hp, blocks * cw), 1)
    spread = jnp.where(row == (col // cw) * hp + lax.rem(col, cw) // hd, 1.0, 0.0).astype(BF)


    @pl.when(kept)
    def _():
        agot(2 * x + 1 - c)

    @pl.when(moved)
    def _():
        afar()

    agot(2 * (1 - x) + 1 - c)
    hgot()

    ocross()
    ofrom(0, middle & moved)
    per = da // kd
    rt = 64

    def norm_rows(parts, r):
        tot = sum(jnp.sum(p * p, axis=-1, keepdims=True) for p in parts)
        rs = lax.rsqrt(tot / (da * T) + EPSILON)
        for t in range(T):
            g = abuf[t, n : n + 1, :].astype(F32)
            v = (parts[t] * rs * g).astype(BF)
            for j in range(per):
                nbuf[t * per + j, r, :] = v[:, j * kd : (j + 1) * kd]

    def norm_tile(i, _):
        r = pl.ds(pl.multiple_of(i * rt, rt), rt)
        norm_rows([abuf[t, r, :].astype(F32) for t in range(T)], r)
        return 0

    lax.fori_loop(0, n // rt, norm_tile, 0)
    norm_rows([hbuf[t].astype(F32) for t in range(T)], pl.ds(n, raw0))
    @pl.when(moved)
    def _():
        pump(1, 1, start)


    mt = 256

    def tiles():
        for r0 in range(0, n, mt):
            yield r0, slice(r0, r0 + mt + raw0 if r0 + mt == n else r0 + mt)

    def keep(ref, r0, low):
        ref[raw0 + r0 : raw0 + r0 + mt, :] = low[0:mt, :].astype(F32)
        if low.shape[0] > mt:
            ref[0:raw0, :] = low[mt:, :].astype(F32)

    for r0, rows in tiles():
        d = jnp.dot(nbuf[0, rows, :], vbuf[0, 0:kd, :], preferred_element_type=F32)
        for i in range(1, S):
            d = d + jnp.dot(nbuf[i, rows, :], vbuf[i, 0:kd, :], preferred_element_type=F32)
        keep(extv, r0, d.astype(BF))

    sacc = bt(vbuf[0, kd:, 0:kd], nbuf[0, 0:n, :])
    for i in range(1, S):
        sacc = sacc + bt(vbuf[i, kd:, 0:kd], nbuf[i, 0:n, :])
    @pl.when(kept)
    def _():
        pump(1, 2, start)

    @pl.when(moved)
    def _():
        pump(1, 2, start, when=middle)

    ofrom(0, jnp.logical_not(middle & moved))

    step = sacc + bias_c
    step = jnp.maximum(step, 0.0) + jnp.log1p(jnp.exp(-jnp.abs(step)))
    ld = rate_c * step + par[0, 0:hp, :]

    def stacked(v):
        return jnp.concatenate([v[:, b * blk : (b + 1) * blk] for b in range(blocks)], axis=0)

    cum_r = jnp.dot(thirds(stacked(ld)), upper, preferred_element_type=F32)
    st_r = stacked(step)
    cum_c = cum_r.T
    grown = jnp.exp(cum_c)
    left = jnp.exp(cum_c[blk - 1 : blk, :] - cum_c) * st_r.T
    both = jnp.dot(thirds(jnp.concatenate([left, grown], axis=0)), spread, preferred_element_type=F32)
    cum_rs, cum_cs, st_rs, wexps = [], [], [], []
    for b in range(blocks):
        expd[b * blk : (b + 1) * blk, :] = both[blk:, b * cw : (b + 1) * cw]
        wexps.append(both[:blk, b * cw : (b + 1) * cw])
        cum_rs.append(cum_r[b * hp : (b + 1) * hp, :])
        cum_cs.append(cum_c[:, b * hp : (b + 1) * hp])
        st_rs.append(st_r[b * hp : (b + 1) * hp, :])


    for b in range(blocks):
        for lo, hi in ((0, cw), (cw, vc)):
            total = jnp.zeros((blk, hi - lo), F32)
            for k in range(width):
                o = b * blk + raw0 - (width - 1) + k
                total = total + par[0, 24 + k : 25 + k, lo:hi] * extv[o : o + blk, lo:hi]
            conv[b * blk : (b + 1) * blk, lo:hi] = (total * jax.nn.sigmoid(total)).astype(BF)

    run = jnp.zeros((st, cw), F32)
    dec = jnp.ones((1, cw), F32)
    pres, offs = [], []
    for b in range(blocks):
        rows = slice(b * blk, (b + 1) * blk)
        key_t = bt(eye_st, conv[rows, cw : cw + st]).astype(BF)
        sv = conv[rows, 0:cw].astype(F32) * wexps[b]
        top, low = halves(sv)
        new = jnp.dot(key_t, top, preferred_element_type=F32) + jnp.dot(key_t, low, preferred_element_type=F32)
        bd = expd[(b + 1) * blk - 1 : (b + 1) * blk, :]
        pres.append(run)
        offs.append(dec)
        run = run * bd + new
        dec = dec * bd

    def inner(b):
        rows = slice(b * blk, (b + 1) * blk)
        g = bt(conv[rows, cw + st :], conv[rows, cw : cw + st])
        for h in range(cw // hd):
            gap = jnp.where(lower, cum_cs[b][:, h : h + 1] - cum_rs[b][h : h + 1, :], -jnp.inf)
            wm = g * jnp.exp(gap) * st_rs[b][h : h + 1, :]
            top, low = halves(wm)
            v = conv[rows, h * hd : (h + 1) * hd]
            scan[rows, h * hd : (h + 1) * hd] = jnp.dot(top, v, preferred_element_type=F32) + jnp.dot(
                low, v, preferred_element_type=F32
            )

    window = lax.shift_left(jnp.int32(2), tp)
    back = (
        lax.broadcasted_iota(jnp.int32, (blk, blk + raw0), 0)
        + raw0
        - lax.broadcasted_iota(jnp.int32, (blk, blk + raw0), 1)
    )
    band = jnp.where((back >= 0) & (back < window), 1.0, 0.0).astype(BF)

    def pool(b):
        rows = slice(b * blk, (b + 1) * blk)
        sums = jnp.dot(band, extp[b * blk : (b + 1) * blk + raw0, :].astype(BF), preferred_element_type=F32)
        pos = (me * n + b * blk + lax.broadcasted_iota(jnp.int32, (blk, cw), 0)).astype(F32)
        counts = jnp.minimum(pos + 1.0, window.astype(F32))
        pooled = (sums / counts - extp[b * blk + raw0 : (b + 1) * blk + raw0, :]).astype(BF)
        pbuf[pslot, rows, :] = (
            jnp.dot(pooled, mixb[0], preferred_element_type=F32) * par[0, 16:17, 0:cw]
        ).astype(BF)

    rows_of = (sbuf, pbuf)

    def rcopy(k, r, way, src=None):
        to = ({"c_": 1 - c}, {"x_": 1 - x}, {"y_": 1 - y})[way]
        src = rows_of[k].at[r] if src is None else src
        return copy(src, rows_of[k].at[r], p_ss.at[(k * T + r) * 3 + way], p_rs.at[k * T + r], **to)

    def qcopy(i):
        to = ({"c_": 1 - c}, {"x_": 1 - x}, {"x_": 1 - x, "c_": 1 - c}, {})[i]
        return copy(sq_buf.at[pslot], sq_buf.at[tp], q_ss.at[i], q_rs.at[tp], **{"y_": c, **to})

    def rows_out(k, do):
        @pl.when(moved)
        def _():
            do(rcopy(k, tp, 2, rows_of[k].at[T]))

        @pl.when(kept)
        def _():
            do(rcopy(k, tp, 1))
            do(rcopy(k, tp, 0))

    def rows_on(k, do, wait=True):
        @pl.when(kept)
        def _():
            other = 2 * x + 1 - y
            if wait:
                rcopy(k, other, 0).wait_recv()
            do(rcopy(k, other, 1))
            do(rcopy(k, other, 0))

    def rows_over(k, do, wait=True):
        @pl.when(kept)
        def _():
            for r in (2 * (1 - x) + y, 2 * (1 - x) + 1 - y):
                if wait:
                    rcopy(k, r, 0).wait_recv()
                do(rcopy(k, r, 0))

    def squares(do):
        for i in range(3):
            do(qcopy(i))

        @pl.when(moved)
        def _():
            do(qcopy(3))

    def gates():
        for r0, rows in tiles():
            d = jnp.dot(nbuf[0, rows, :], gbuf[0], preferred_element_type=F32)
            for i in range(1, S):
                d = d + jnp.dot(nbuf[i, rows, :], gbuf[i], preferred_element_type=F32)
            low = d.astype(BF)
            keep(extp, r0, low[:, 0:cw])
            gateb[r0 : r0 + mt, :] = low[0:mt, cw:]

    def pools():
        for b in range(blocks):
            pool(b)
        rows_out(1, start)

    def xpair():
        return copy(xs.at[0], xr.at[Z - 1], x_ss.at[0], x_rs.at[Z - 1], c_=1 - c)

    def lanes(who):
        return pl.ds(pl.multiple_of(who * (cw // 2), cw // 2), cw // 2)

    def xline(k):
        return copy(xs.at[1, :, lanes(c)], xr.at[z, :, lanes(c)], x_ss.at[k], x_rs.at[z], z_=z + k)

    def xshare(p, who):
        ref = xr.at[p, :, lanes(who)]
        return copy(ref, ref, x_ss.at[Z + p], x_rs.at[Z + p], c_=1 - c)

    def xshares(do):
        for p in range(Z - 1):
            @pl.when(z > p)
            def _():
                do(p)

    def xgot(p):
        ref = xr.at[p, :, lanes(c)]
        copy(ref, ref, x_ss.at[1], x_rs.at[p], c_=1 - c).wait_recv()
        xshare(p, c).start()

    def xlines(do):
        for k in range(1, Z):
            @pl.when(z + k < Z)
            def _():
                do(xline(k))

    def put(i):
        xs[i, 0:st, :] = run
        xs[i, st:, :] = jnp.broadcast_to(dec, (xs.shape[1] - st, cw))

    put(0)
    xpair().start()

    @pl.when(kept)
    def _():
        pump(1, 3, start)

    @pl.when(moved)
    def _():
        pump(1, 2, start, when=jnp.logical_not(middle))

    for b in range(blocks // 2):
        inner(b)
    xpair().wait_recv()
    other, odec = xr[Z - 1, 0:st, :], xr[Z - 1, st : st + 1, :]
    later = c == 1
    own_s, own_d = jnp.where(later, other, 0.0), jnp.where(later, odec, 1.0)
    run = jnp.where(later, other * dec + run, run * odec + other)
    dec = dec * odec
    put(1)
    xlines(start)
    ofrom(1, middle)

    for b in range(blocks // 2, blocks):
        inner(b)
    opass(0, kept)

    @pl.when(moved)
    def _():
        pump(1, 3, start)

    ofrom(1, jnp.logical_not(middle))
    partners(1)
    gates()

    @pl.when(moved)
    def _():
        swap(3).wait_recv()

    pools()
    opass(0, moved)
    xshares(xgot)
    in_s = jnp.zeros((st, cw), F32)
    for p in range(Z - 1):
        @pl.when(z > p)
        def _():
            xshare(p, 1 - c).wait_recv()

        in_s = jnp.where(z > p, in_s * xr[p, st : st + 1, :] + xr[p, 0:st, :], in_s)
    in_s = in_s * own_d + own_s

    for b in range(blocks):
        rows = slice(b * blk, (b + 1) * blk)
        top, low = halves(pres[b] + offs[b] * in_s)
        rd = conv[rows, cw + st :]
        carried = jnp.dot(rd, top, preferred_element_type=F32) + jnp.dot(rd, low, preferred_element_type=F32)
        out_b = scan[rows, :] + carried * expd[rows, :] + skips * conv[rows, 0:cw].astype(F32)
        gt = gateb[rows, :].astype(F32)
        gated = out_b * (gt * jax.nn.sigmoid(gt))
        sq_buf[pslot, :, rows] = bt(jnp.ones((8, cw), F32), gated * gated, precision=HIGH)
        sbuf[pslot, rows, :] = (gated * par[0, 16:17, cw : 2 * cw]).astype(BF)

    rows_out(0, start)
    squares(start)
    olate(0)
    opass(1)
    olate(1)
    oend(0)
    rows_on(1, start)
    ofar(0, start)
    oend(1)
    rows_on(0, start)
    if TWIN:
        otwin(0, start)
    ofar(1, start)
    rows_over(1, start)
    if TWIN > 1:
        otwin(1, start)
    def rows_here(k):
        @pl.when(moved)
        def _():
            for r in range(T):
                rcopy(k, r, 0).wait_recv()

    def product(k, family, rows):
        part = slice(cw, 2 * cw) if k == 0 else slice(0, cw)
        p = jnp.dot(rows_of[k][0, rows, :], obuf[family * T, part, :], preferred_element_type=F32)
        for q in range(1, T):
            p = p + jnp.dot(rows_of[k][q, rows, :], obuf[family * T + q, part, :], preferred_element_type=F32)
        return p

    def spots(family):
        return pl.ds(pl.multiple_of(family * oc, oc), oc)

    rows_here(1)
    for r0 in range(0, n, mt):
        scan[r0 : r0 + mt, 0:oc] = product(1, y, slice(r0, r0 + mt))
    rows_over(0, start)
    rows_here(0)
    for r in range(T):
        @pl.when((tp != r) | moved)
        def _():
            copy(sq_buf.at[r], sq_buf.at[r], q_ss.at[0], q_rs.at[r], c_=1 - c).wait_recv()

    sq = sum(sq_buf[r] for r in range(T))
    rs_row = lax.rsqrt(sq / (cw * T) + EPSILON)
    rs_cols = [bt(eye, rs_row[:, b * blk : (b + 1) * blk], precision=HIGH)[:, 0:1] for b in range(blocks)]

    def scales(r0):
        return jnp.concatenate(rs_cols[r0 // blk : (r0 + mt) // blk], axis=0)

    for r0 in range(0, n, mt):
        rows = slice(r0, r0 + mt)
        out[rows, spots(y)] = (scan[rows, 0:oc] + scales(r0) * product(0, y, rows)).astype(out.dtype)

    for q in range(T):
        i = (1 - y) * T + q
        known = (q == 2 * x + 1 - y) & (TWIN > 0) | (q == 2 * x + y) & (TWIN > 1)

        @pl.when(jnp.logical_not(relays(0) & known))
        def _():
            copy(obuf.at[i], obuf.at[i], o_ss.at[0], o_rs.at[i], y_=1 - y).wait_recv()

    for r0 in range(0, n, mt):
        rows = slice(r0, r0 + mt)
        p = product(1, 1 - y, rows)
        out[rows, spots(1 - y)] = (p + scales(r0) * product(0, 1 - y, rows)).astype(out.dtype)

    for k in range(2):
        source(k, done)
        for d in range(1, Z):
            pump(k, d, done, wait=False)
        rows_out(k, done)
        rows_on(k, done, wait=False)
        rows_over(k, done, wait=False)
    oall(done)
    squares(done)
    acopy(1).wait_send()
    acopy(2).wait_send()

    @pl.when(moved)
    def _():
        acopy(0).wait_send()
        for i in range(4):
            swap(i).wait_send()
        aforward(0).wait_send()
        aforward(2).wait_send()

    @pl.when(kept)
    def _():
        aforward(1).wait_send()

    @pl.when(jnp.logical_not(hub))
    def _():
        ohub().wait_send()

    xpair().wait_send()
    xlines(done)
    xshares(lambda p: xshare(p, c).wait_send())

    hsends(done)


def fits(S, T, shapes):
    n, da = shapes[0]
    kd, cw = shapes[2]
    st = shapes[5][1]
    oc = shapes[18][1]
    heads = shapes[7][1]
    taps = shapes[10][0]
    return (
        T == 4 == POOL_GROUPS and S == 2 * T and st == SSM_STATE and taps <= 8 and heads <= 8
        and cw == heads * SSM_STATE and n % 256 == 0 and n % SCAN_BLOCK == 0 and n >= 2 * cw
        and oc % 128 == 0 and kd % 128 == 0 and da % kd == 0 and da * T == kd * S and kd <= cw + 2 * st
        and cw % 256 == 0 and oc * 2 == da and oc <= cw
    )


def fused(
    S, T, activations, norm_gain, pool_weight, gate_weight, value_weight, key_weight, read_weight,
    step_weight, pool_mix, pool_scale, taps_value, taps_key, taps_read, step_bias, decay_log,
    decay_extra, skip_scale, state_gain, out_pool_weight, out_state_weight,
):
    n, da = activations.shape
    kd, cw = pool_weight.shape
    st = key_weight.shape[1]
    oc = out_pool_weight.shape[1]
    hp = 16
    args = (
        activations, norm_gain.reshape(-1, 128), pool_weight, gate_weight, value_weight, key_weight.T, read_weight.T,
        step_weight.T, pool_mix, pool_scale[None, :], taps_value, taps_key, taps_read, step_bias[None, :], decay_log[None, :],
        decay_extra.T, skip_scale[None, :], state_gain[None, :],
        out_pool_weight, out_state_weight,
    )
    vc = cw + 2 * st
    V = pltpu.VMEM
    D = pltpu.SemaphoreType.DMA
    scratch = [
        V((S + 1, kd + hp, vc), BF), V((S + 1, kd, 2 * cw), BF), V((2 * T + 3, 2 * cw, oc), BF),
        V((T + 1, n + 16, da), BF), V((2, cw, cw), BF), V((2, 32, n), F32),
        V((S, n + 16, kd), BF), V((n + 16, vc), F32), V((n + 16, cw), F32), V((n, cw), BF), V((n, vc), BF),
        V((T, 16, da), BF), V((n, cw), F32),
        V((2, st + 8, cw), F32), V((S // 2, st + 8, cw), F32),
        V((T + 1, 8, n), F32), V((T + 1, n, cw), BF), V((T + 1, n, cw), BF), V((n, cw), F32),
        D((10 * S,)), D((2 * S,)), D((29,)), D((2 * T + 3,)), D((6,)), D((T + 1,)), D((4,)), D((2,)),
        D((4,)), D((T,)), D((S,)), D((S,)), D((4,)), D((T,)), D((6 * T,)), D((2 * T,)),
    ]
    return pl.pallas_call(
        functools.partial(mixer_kernel, S, T),
        out_shape=jax.ShapeDtypeStruct((n, da), BF),
        in_specs=[pl.BlockSpec(memory_space=pltpu.VMEM)] * len(args),
        out_specs=pl.BlockSpec(memory_space=pltpu.VMEM),
        scratch_shapes=scratch,
        compiler_params=pltpu.CompilerParams(
            collective_id=0, has_side_effects=True, vmem_limit_bytes=60 * 1024 * 1024
        ),
    )(*args)


def solution(mesh):
    placed = (
        P("sp", "tp"),
        P("tp"),
        P("sp", "tp"),
        P("sp", "tp"),
        P("sp", "tp"),
        P("sp", "tp"),
        P("sp", "tp"),
        P("sp", "tp"),
        P("tp", None, None),
        P("tp"),
        P(None, "tp"),
        P(None, "tp"),
        P(None, "tp"),
        P("tp"),
        P("tp"),
        P("sp", "tp"),
        P("tp"),
        P("tp"),
        P("tp", "sp"),
        P("tp", "sp"),
    )
    S, T = mesh.shape["sp"], mesh.shape["tp"]

    def chosen(*args):
        if fits(S, T, [a.shape for a in args]):
            return fused(S, T, *args)
        return local(*args)

    return jax.shard_map(
        chosen, mesh=mesh, in_specs=placed, out_specs=P("sp", "tp"), check_vma=False
    )
```
